32 devices in a mesh: grp: 2 (over y), sp: 4 (over z), tp: 4 (over x, core).
Axes of the slice: x: 2, y: 2, z: 4, core: 2. Of those that a mesh axis runs over, the one named last changes fastest.
Arguments:
- resid_in: bfloat16 [2048, 2048], P(('grp', 'sp', 'tp')), parts along dimension 0, may hold values from -6 to 6
- query_narrow: bfloat16 [2048, 8, 128], P(('grp', 'sp'), 'tp'), parts along dimension 0, may hold values from -512 to 512
- key_narrow: bfloat16 [2048, 4, 128], P(('grp', 'sp'), 'tp'), parts along dimension 0, may hold values from -512 to 512
- value_narrow: bfloat16 [2048, 4, 128], P(('grp', 'sp'), 'tp'), parts along dimension 0, may hold values from -6 to 6
- query_wide: bfloat16 [2048, 8, 256], P(('grp', 'sp'), 'tp'), parts along dimension 0, may hold values from -512 to 512
- key_wide: bfloat16 [2048, 4, 256], P(('grp', 'sp'), 'tp'), parts along dimension 0, may hold values from -512 to 512
- value_wide: bfloat16 [2048, 4, 128], P(('grp', 'sp'), 'tp'), parts along dimension 0, may hold values from -6 to 6
- lambda_narrow: float32 [8], P('tp'), may hold values from 0.3 to 0.8
- lambda_wide: float32 [8], P('tp'), may hold values from 0.3 to 0.8
- head_gain: float32 [128], replicated, may hold values from 0.1 to 1.9
- out_narrow: bfloat16 [1024, 2048], P('tp'), may hold values from -0.125 to 0.125
- out_wide: bfloat16 [1024, 2048], P('tp'), may hold values from -0.125 to 0.125
- norm_gain: bfloat16 [2048], replicated, may hold values from 0.099609375 to 1.8984375
- up_weight: bfloat16 [2048, 8192], P('sp', 'tp'), may hold values from -0.125 to 0.125
- down_weight: bfloat16 [8192, 2048], P('tp', 'sp'), may hold values from -0.0625 to 0.0625
Outputs:
- mixed_out: bfloat16 [2048, 2048], P(('grp', 'sp', 'tp')), parts along dimension 0
The draws below stay inside these ranges and needn't reach their ends.
There are 2 independent parts, one for each index of `grp`. The reference program is written for one: setup_inputs(seed, part) draws one part's arguments, and reference() takes and returns one part's arrays. A program takes and returns all parts, laid end to end along the dimension named above; an argument that names none is the same for every part. Nothing has to cross between parts.
All inputs are finite; a program needn't handle non-finite values.
Results may differ from the reference program's by a relative error of at most 0.018.
Values may be sent and summed in bfloat16 or wider, within the bound.
A program may use at most 128 MiB of HBM per device.

```python
import math
import jax
import jax.numpy as jnp
from jax import lax

D = 2048
FF = 8192
HN = 8
DN = 64
KN = 4
HW = 8
DW = 128
KW = 4
DV = 128
SEQ = 1024
N_TP = 4


SPREAD = 1.32


def paired_draw(base_key, head_count, key_head_stack, half_width):
    full_width = 2 * half_width
    query_draw, keys_draw = jax.random.split(base_key, 2)
    key_rows = jnp.clip(jax.random.normal(keys_draw, (SEQ, key_head_stack, full_width), jnp.float32) * SPREAD, -4.0 * SPREAD, 4.0 * SPREAD)
    query_rows_all = jnp.clip(jax.random.normal(query_draw, (SEQ, head_count, full_width), jnp.float32) * SPREAD, -4.0 * SPREAD, 4.0 * SPREAD)
    return (query_rows_all, key_rows)


def draw_query_narrow(key, part):
    return paired_draw(jax.random.fold_in(key, 101), HN, KN, DN)[0].astype(jnp.bfloat16)


def draw_key_narrow(key, part):
    return paired_draw(jax.random.fold_in(key, 101), HN, KN, DN)[1].astype(jnp.bfloat16)


def draw_query_wide(key, part):
    return paired_draw(jax.random.fold_in(key, 202), HW, KW, DW)[0].astype(jnp.bfloat16)


def draw_key_wide(key, part):
    return paired_draw(jax.random.fold_in(key, 202), HW, KW, DW)[1].astype(jnp.bfloat16)


def steps_of(rng, shape, cuts, smallest, high):
    level = 1.0
    for dim, shards_of in cuts:
        steps = jax.random.uniform(jax.random.fold_in(jax.random.fold_in(rng, 6), dim), (shards_of,), jnp.float32, smallest / len(cuts), high / len(cuts))
        level = level * jnp.repeat(jnp.exp(steps), shape[dim] // shards_of).reshape((-1,) + (1,) * (len(shape) - 1 - dim))
    return level


def scatter_about(key, dims, spread, limit, cuts=(), held_as=jnp.bfloat16):
    result = jax.random.normal(key, dims, jnp.float32) * spread
    if len(cuts) > 0:
        result = steps_of(key, dims, cuts, -0.22, 0.18) * result
    return jnp.clip(result, min=-limit, max=limit).astype(held_as)


def setup_inputs(seed: int = 0, part: int = 0) -> dict:
    streams_of = jax.random.split(jax.random.key(seed), 16)
    part_splits = jax.random.split(jax.random.fold_in(streams_of[15], part), 16)
    return {
        "resid_in": scatter_about(part_splits[0], (SEQ, D), 1.0, 6.0, ((0, 16),)),
        "query_narrow": draw_query_narrow(jax.random.fold_in(jax.random.fold_in(streams_of[15], part), 71), part),
        "key_narrow": draw_key_narrow(jax.random.fold_in(jax.random.fold_in(streams_of[15], part), 71), part),
        "value_narrow": scatter_about(part_splits[3], (SEQ, KN, DV), 1.0, 6.0, ((0, 4), (1, 4))),
        "query_wide": draw_query_wide(jax.random.fold_in(jax.random.fold_in(streams_of[15], part), 71), part),
        "key_wide": draw_key_wide(jax.random.fold_in(jax.random.fold_in(streams_of[15], part), 71), part),
        "value_wide": scatter_about(part_splits[6], (SEQ, KW, DV), 1.0, 6.0, ((0, 4), (1, 4))),
        "lambda_narrow": jnp.clip(0.3 + 0.5 * jax.random.uniform(streams_of[7], (HN,), jnp.float32) ** steps_of(streams_of[7], (HN,), ((0, 4),), -0.2, 0.2), 0.3, 0.8),
        "lambda_wide": jnp.clip(0.3 + 0.5 * jax.random.uniform(streams_of[8], (HW,), jnp.float32) ** steps_of(streams_of[8], (HW,), ((0, 4),), -0.2, 0.2), 0.3, 0.8),
        "head_gain": jnp.clip(1.0 + 0.18 * jax.random.normal(streams_of[9], (DV,), jnp.float32), 0.1, 1.9),
        "out_narrow": scatter_about(streams_of[10], (HN * DV, D), ((HN + HW) * DV) ** -0.5, 0.125, ((0, 4),)),
        "out_wide": scatter_about(streams_of[11], (HW * DV, D), ((HN + HW) * DV) ** -0.5, 0.125, ((0, 4),)),
        "norm_gain": jnp.clip(1.0 + 0.18 * jax.random.normal(streams_of[12], (D,), jnp.float32), 0.099609375, 1.8984375).astype(jnp.bfloat16),
        "up_weight": scatter_about(streams_of[13], (D, FF), D ** -0.5, 0.125, ((0, 4), (1, 4))),
        "down_weight": scatter_about(streams_of[14], (FF, D), FF ** -0.5, 0.0625, ((0, 4), (1, 4))),
    }


NORM_EPS = 1e-06
OUT_SCALE = 0.8

def attend_ref(query, key_rows, values, lambdas, gain_vec):
    seq_len, head_count, full_width = query.shape
    key_head_stack = key_rows.shape[1]
    half_width = full_width // 2
    group_size = head_count // key_head_stack
    value_width = values.shape[2]
    block_rows = math.gcd(seq_len, 128)
    rotation_count = seq_len // block_rows
    key_float32 = key_rows.astype(jnp.float32).reshape(seq_len, key_head_stack, 2, half_width)
    value_float32 = values.astype(jnp.float32)
    query_blocks = query.reshape(rotation_count, block_rows, key_head_stack, group_size, 2, half_width)
    lambda_grid = lambdas.reshape(key_head_stack, group_size)[:, :, None, None]

    def per_block(query_blk):
        scores = jnp.einsum('tkgcd,skcd->kgcts', query_blk.astype(jnp.float32), key_float32) * half_width ** (-0.5)
        row_top = lax.optimization_barrier(jnp.max(scores, axis=-1, keepdims=True))
        powers = jnp.exp(scores - row_top)
        row_total = lax.optimization_barrier(jnp.sum(powers, axis=-1))
        rounded_result = lax.optimization_barrier(powers.astype(jnp.bfloat16)).astype(jnp.float32)
        weighted_values = jnp.einsum('iodph,hie->iodpe', rounded_result, value_float32)
        first_map = weighted_values[:, :, 0] / row_total[:, :, 0, :, None]
        second_map = weighted_values[:, :, 1] / row_total[:, :, 1, :, None]
        mixed = first_map - lambda_grid * second_map
        normed = mixed * lax.rsqrt(lax.optimization_barrier(jnp.mean(mixed * mixed, axis=-1, keepdims=True)) + NORM_EPS) * gain_vec * OUT_SCALE
        normed = normed.astype(jnp.bfloat16).transpose(2, 0, 1, 3)
        return normed.reshape(block_rows, head_count, value_width)
    outcome = lax.map(per_block, query_blocks)
    return outcome.reshape(seq_len, head_count * value_width)

def rounded_add(running, partial_value):
    return running + lax.optimization_barrier(partial_value.astype(jnp.bfloat16)).astype(jnp.float32)

def reference(resid_in, query_narrow, key_narrow, value_narrow, query_wide, key_wide, value_wide, lambda_narrow, lambda_wide, head_gain, out_narrow, out_wide, norm_gain, up_weight, down_weight):
    att_narrow = attend_ref(query_narrow, key_narrow, value_narrow, lambda_narrow, head_gain)
    att_wide = attend_ref(query_wide, key_wide, value_wide, lambda_wide, head_gain)
    narrow_cols = att_narrow.shape[1] // N_TP
    wide_cols = att_wide.shape[1] // N_TP
    projected = jnp.zeros(resid_in.shape, jnp.float32)
    for part_index in range(N_TP):
        low_n = part_index * narrow_cols
        low_w = part_index * wide_cols
        partial_value = jnp.dot(att_narrow[:, low_n:low_n + narrow_cols], out_narrow[low_n:low_n + narrow_cols], preferred_element_type=jnp.float32)
        partial_value = partial_value + jnp.dot(att_wide[:, low_w:low_w + wide_cols], out_wide[low_w:low_w + wide_cols], preferred_element_type=jnp.float32)
        projected = rounded_add(projected, partial_value)
    middle = (resid_in.astype(jnp.float32) + projected).astype(jnp.bfloat16)
    middle_f32 = middle.astype(jnp.float32)
    normed = middle_f32 * lax.rsqrt(lax.optimization_barrier(jnp.mean(middle_f32 * middle_f32, axis=-1, keepdims=True)) + NORM_EPS)
    normed = (normed * norm_gain.astype(jnp.float32)).astype(jnp.bfloat16)
    hidden_cols = up_weight.shape[1] // N_TP
    mixer = jnp.zeros(resid_in.shape, jnp.float32)
    for part_index in range(N_TP):
        low_h = part_index * hidden_cols
        lifted = jnp.dot(normed, up_weight[:, low_h:low_h + hidden_cols], preferred_element_type=jnp.float32)
        activated = jnp.square(jax.nn.relu(lifted)).astype(jnp.bfloat16)
        partial_value = jnp.dot(activated, down_weight[low_h:low_h + hidden_cols], preferred_element_type=jnp.float32)
        mixer = rounded_add(mixer, partial_value)
    return (middle_f32 + mixer).astype(jnp.bfloat16)
```

```python
import math

import jax
import jax.numpy as jnp
from jax import lax
from jax.experimental import pallas as pl
from jax.experimental.pallas import tpu as pltpu
from jax.sharding import PartitionSpec as P

NORM_EPS = 1e-06
OUT_SCALE = 0.8


def empty_state(query, key_head_stack, value_width):
    row_count, head_count = (query.shape[0], query.shape[1])
    group_size = head_count // key_head_stack
    row_top = jnp.full((key_head_stack, group_size, 2, row_count), -jnp.inf, jnp.float32)
    row_total = jnp.zeros((key_head_stack, group_size, 2, row_count), jnp.float32)
    weighted_values = jnp.zeros(
        (key_head_stack, group_size, 2, row_count, value_width), jnp.float32
    )
    return (row_top, row_total, weighted_values)


def absorb(states, query, key_rows, values):
    row_count, head_count = (query.shape[0], query.shape[1])
    key_head_stack = key_rows.shape[1]
    half_width = key_rows.shape[2] // 2
    group_size = head_count // key_head_stack
    value_width = values.shape[2]
    amount = key_rows.shape[0]
    block_rows = math.gcd(amount, 512)
    rotation_count = amount // block_rows
    grouped = query.reshape(row_count, key_head_stack, group_size, 2, half_width)
    key_block_list = key_rows.reshape(rotation_count, block_rows, key_head_stack, 2, half_width)
    value_blocks = values.reshape(rotation_count, block_rows, key_head_stack, value_width)

    def visit(running, kv_pair):
        row_top, row_total, weighted_values = running
        key_blk, value_blk = kv_pair
        scores = jnp.einsum(
            "tkgcd,skcd->kgcts", grouped, key_blk, preferred_element_type=jnp.float32
        ) * half_width ** (-0.5)
        new_top = jnp.maximum(row_top, jnp.max(scores, axis=-1))
        rescale = jnp.exp(row_top - new_top)
        powers = jnp.exp(scores - new_top[..., None])
        row_total = row_total * rescale + jnp.sum(powers, axis=-1)
        weighted_values = weighted_values * rescale[..., None] + jnp.einsum(
            "iodph,hie->iodpe",
            powers.astype(jnp.bfloat16),
            value_blk,
            preferred_element_type=jnp.float32,
        )
        return ((new_top, row_total, weighted_values), None)

    outcome, _ = lax.scan(visit, states, (key_block_list, value_blocks))
    return outcome


def finish(states, lambdas, gain_vec):
    row_top, row_total, weighted_values = states
    key_head_stack, group_size, row_count = (row_top.shape[0], row_top.shape[1], row_top.shape[3])
    value_width = weighted_values.shape[4]
    first_map = weighted_values[:, :, 0] / row_total[:, :, 0, :, None]
    second_map = weighted_values[:, :, 1] / row_total[:, :, 1, :, None]
    mixed = first_map - lambdas.reshape(key_head_stack, group_size)[:, :, None, None] * second_map
    normed = (
        mixed
        * lax.rsqrt(jnp.mean(mixed * mixed, axis=-1, keepdims=True) + NORM_EPS)
        * gain_vec
        * OUT_SCALE
    )
    normed = normed.astype(jnp.bfloat16).transpose(2, 0, 1, 3)
    return normed.reshape(row_count, key_head_stack * group_size * value_width)


def attend(
    query_narrow,
    key_narrow,
    value_narrow,
    query_wide,
    key_wide,
    value_wide,
    lambda_narrow,
    lambda_wide,
    head_gain,
):
    initial = (
        empty_state(query_narrow, key_narrow.shape[1], value_narrow.shape[2]),
        empty_state(query_wide, key_wide.shape[1], value_wide.shape[2]),
    )
    narrow_keys = lax.all_gather(key_narrow, "sp", axis=0, tiled=True)
    narrow_values = lax.all_gather(value_narrow, "sp", axis=0, tiled=True)
    wide_keys = lax.all_gather(key_wide, "sp", axis=0, tiled=True)
    wide_values = lax.all_gather(value_wide, "sp", axis=0, tiled=True)
    narrow_state = absorb(initial[0], query_narrow, narrow_keys, narrow_values)
    wide_state = absorb(initial[1], query_wide, wide_keys, wide_values)
    return (
        finish(narrow_state, lambda_narrow, head_gain),
        finish(wide_state, lambda_wide, head_gain),
    )


def shards(
    resid_in,
    query_narrow,
    key_narrow,
    value_narrow,
    query_wide,
    key_wide,
    value_wide,
    lambda_narrow,
    lambda_wide,
    head_gain,
    out_narrow,
    out_wide,
    norm_gain,
    up_weight,
    down_weight,
):
    att_narrow, att_wide = attend(
        query_narrow,
        key_narrow,
        value_narrow,
        query_wide,
        key_wide,
        value_wide,
        lambda_narrow,
        lambda_wide,
        head_gain,
    )
    projected = lax.psum_scatter(
        (
            jnp.dot(att_narrow, out_narrow, preferred_element_type=jnp.float32)
            + jnp.dot(att_wide, out_wide, preferred_element_type=jnp.float32)
        ).astype(jnp.bfloat16),
        "tp",
        scatter_dimension=0,
        tiled=True,
    ).astype(jnp.float32)
    middle = (resid_in.astype(jnp.float32) + projected).astype(jnp.bfloat16)
    middle_f32 = middle.astype(jnp.float32)
    normed = middle_f32 * lax.rsqrt(
        jnp.mean(middle_f32 * middle_f32, axis=-1, keepdims=True) + NORM_EPS
    )
    normed = (normed * norm_gain.astype(jnp.float32)).astype(jnp.bfloat16)
    whole_rows = lax.all_gather(normed, "tp", axis=0, tiled=True)
    up_collected = lax.all_gather(up_weight, "sp", axis=0, tiled=True)
    lifted = jnp.dot(whole_rows, up_collected, preferred_element_type=jnp.float32)
    activated = jnp.square(jax.nn.relu(lifted)).astype(jnp.bfloat16)
    partials = jnp.dot(
        activated,
        lax.all_gather(down_weight, "sp", axis=1, tiled=True),
        preferred_element_type=jnp.float32,
    )
    mixer_out = lax.psum_scatter(
        partials.astype(jnp.bfloat16), "tp", scatter_dimension=0, tiled=True
    ).astype(jnp.float32)
    return (middle_f32 + mixer_out).astype(jnp.bfloat16)


LOG2E = math.log2(math.e)
VMEM_BYTES = 60 * 2**20


def dot32(a, b):
    return jnp.dot(a, b, preferred_element_type=jnp.float32)


def layer_kernel(plan, resid_in, qn_in, kn_in, vn_in, qw_in, kw_in, vw_in, lam_n, lam_w, head_gain,
                 outn_in, outw_in, norm_gain, up, down,
                 out, qn, qw, resid, out_n, out_w, kv_full, att, proj, core_in, x_out, x_in, middle, act,
                 hidden, up_full, down_full, part, core_recv, x_send, x_recv, z_send, z_recv, total,
                 local, kv_ss, kv_rs, wz_ss, wz_rs, wy_ss, wy_rs, pc_ss, pc_rs, px_ss, px_rs,
                 az_ss, az_rs, ax_ss, ax_rs, ac_ss, ac_rs, rc_ss, rc_rs, rx_ss, rx_rs, rz_ss, rz_rs):
    grp_n, sp_n, tp_n, spots, maps = plan
    g, s, t = lax.axis_index("grp"), lax.axis_index("sp"), lax.axis_index("tp")
    rows = qn.shape[0]
    mine, width = resid.shape
    deep = up.shape[0]
    hid = up_full.shape[1]
    f32, bf16 = jnp.float32, jnp.bfloat16
    x_peer = lax.rem(t + 2, tp_n)
    c_peer = t + 1 - 2 * lax.rem(t, 2)
    cx_peer = lax.rem(c_peer + 2, tp_n)
    y_peer = 1 - g

    nearest = [sorted(range(sp_n), key=lambda p: (abs(p - me), p)) for me in range(sp_n)]

    def plane(i):
        at = nearest[0][i]
        for me in range(1, sp_n):
            at = jnp.where(s == me, nearest[me][i], at)
        return at

    planes = [s] + [plane(i) for i in range(1, sp_n)]

    def send(src, dst, ss, rs, dev):
        return pltpu.make_async_remote_copy(
            src_ref=src, dst_ref=dst, send_sem=ss, recv_sem=rs,
            device_id=dev, device_id_type=pl.DeviceIdType.MESH)

    def cols_of(p):
        return pl.ds(pl.multiple_of(p * deep, 128), deep)

    loads = []

    def load(src, dst):
        copy = pltpu.make_async_copy(src, dst, local.at[len(loads)])
        copy.start()
        loads.append(copy)

    own = pl.ds(s * rows, rows)
    for ref, (at, size) in zip((kn_in, vn_in, kw_in, vw_in), spots):
        load(ref, kv_full.at[own, at:at + size])
    load(qn_in, qn)
    load(qw_in, qw)
    load(outn_in, out_n)
    load(outw_in, out_w)
    load(resid_in, resid)
    load(up.at[:, pl.ds(pl.multiple_of(s * hid, 128), hid)], up_full.at[pl.ds(s * deep, deep)])
    load(down.at[pl.ds(s * hid, hid)], down_full.at[:, cols_of(s)])

    barrier = pltpu.get_barrier_semaphore()
    peers = [{"sp": lax.rem(s + d, sp_n)} for d in range(1, sp_n)]
    peers += [{"tp": x_peer}, {"tp": c_peer}, {"grp": y_peer}]
    for peer in peers:
        pl.semaphore_signal(barrier, inc=1, device_id=peer, device_id_type=pl.DeviceIdType.MESH)
    for copy in loads[:4]:
        copy.wait()
    pl.semaphore_wait(barrier, len(peers))

    half_d, half_h = deep // grp_n, hid // grp_n

    def weight_send(kind, i):
        to = planes[i]
        if kind == 0:
            return send(up.at[pl.ds(g * half_d, half_d), pl.ds(pl.multiple_of(to * hid, 128), hid)],
                        up_full.at[pl.ds(s * deep + g * half_d, half_d)],
                        wz_ss.at[0, i], wz_rs.at[0, s], {"sp": to})
        return send(down.at[pl.ds(to * hid + g * half_h, half_h)],
                    down_full.at[pl.ds(g * half_h, half_h), cols_of(s)],
                    wz_ss.at[1, i], wz_rs.at[1, s], {"sp": to})

    def weight_ref(kind, i):
        at = planes[i]
        if kind == 0:
            return up_full.at[pl.ds(at * deep + g * half_d, half_d)]
        return down_full.at[pl.ds(g * half_h, half_h), cols_of(at)]

    def weight_pass(kind, i):
        ref = weight_ref(kind, i)
        return send(ref, ref, wy_ss.at[kind, i], wy_rs.at[kind, i], {"grp": y_peer})

    def weights_out(kind, way):
        for i in range(1, sp_n):
            @pl.when((planes[i] > s) if way == 1 else (planes[i] < s))
            def _():
                weight_send(kind, i).start()

    def weights_on(kind, i):
        ref = weight_ref(kind, i)
        send(ref, ref, wz_ss.at[kind, i], wz_rs.at[kind, planes[i]], {"sp": planes[i]}).wait_recv()
        weight_pass(kind, i).start()

    def passes(k, way):
        return (s >= k) & (s < sp_n - 1) if way == 1 else (s <= sp_n - 1 - k) & (s > 0)

    def comes(k, way):
        return (s >= k) if way == 1 else (s <= sp_n - 1 - k)

    def last(k, way):
        return (s == k) if way == 1 else (s == sp_n - 1 - k)

    def kv_pass(k, way):
        at = kv_full.at[pl.ds((s - way * k) * rows, rows)]
        lane = (1 - way) // 2
        return send(at, at, kv_ss.at[lane, k], kv_rs.at[lane, k], {"sp": s + way})

    def kv_come(k, way):
        at = kv_full.at[pl.ds((s - way * k) * rows, rows)]
        lane = (1 - way) // 2
        return send(at, at, kv_ss.at[lane, k - 1], kv_rs.at[lane, k - 1], {"sp": s - way})

    for k in range(sp_n):
        for way in (1, -1):
            if k:
                @pl.when(comes(k, way))
                def _():
                    kv_come(k, way).wait_recv()

            @pl.when(passes(k, way))
            def _():
                kv_pass(k, way).start()

            @pl.when(last(k, way))
            def _():
                weights_out(0, way)

    for copy in loads[4:]:
        copy.wait()

    lane = lax.broadcasted_iota(jnp.int32, (rows, 128), 1)
    for kind, ref in enumerate((qn, qw)):
        queries = ref[...].astype(f32)
        for h, (order, kh, half, k_at, v_at) in enumerate(maps[kind]):
            lam = (lam_n if kind == 0 else lam_w)[h]
            query = queries[:, h, :]
            vals = kv_full[:, v_at:v_at + head_gain.shape[0]]
            sides = []
            for c in range(2):
                if half % 128:
                    part_q = jnp.where((lane // half) == c, query, 0.0)
                    keys = kv_full[:, k_at:k_at + 2 * half]
                else:
                    part_q = query[:, c * half:(c + 1) * half]
                    keys = kv_full[:, k_at + c * half:k_at + (c + 1) * half]
                scores = lax.dot_general(
                    part_q.astype(bf16), keys, (((1,), (1,)), ((), ())), preferred_element_type=f32)
                top = jnp.max(scores, axis=-1, keepdims=True)
                powers = jnp.exp2((scores - top) * (half ** -0.5 * LOG2E))
                row_total = jnp.sum(powers, axis=-1, keepdims=True)
                sides.append(dot32(powers.astype(bf16), vals) / row_total)
            mixed = sides[0] - lam * sides[1]
            v_width = mixed.shape[1]
            normed = (mixed * lax.rsqrt(jnp.mean(mixed * mixed, axis=-1, keepdims=True) + NORM_EPS)
                      * head_gain[...][None] * OUT_SCALE)
            att[:, order * v_width:(order + 1) * v_width] = normed.astype(bf16)

    cut = out_n.shape[0]
    chunk = math.gcd(width, 512)
    n_half = width // 2

    def row_block(who):
        return pl.ds(who * mine, mine)

    pc = {}
    for j in range(2):
        cols = slice(j * n_half, (j + 1) * n_half)
        for at in range(j * n_half, (j + 1) * n_half, chunk):
            some = slice(at, at + chunk)
            proj[:, some] = (dot32(att[:, :cut], out_n[:, some]) + dot32(att[:, cut:], out_w[:, some])).astype(bf16)
        for i, who in enumerate((cx_peer, c_peer)):
            pc[j, i] = send(proj.at[row_block(who), cols], core_in.at[i, :, cols],
                            pc_ss.at[j, i], pc_rs.at[j, i], {"tp": c_peer})
            pc[j, i].start()
    weights_on(0, 1)
    px = []
    for j in range(2):
        cols = slice(j * n_half, (j + 1) * n_half)
        pc[j, 0].wait_recv()
        x_out[:, cols] = (proj[row_block(x_peer), cols].astype(f32) + core_in[0, :, cols].astype(f32)).astype(bf16)
        px.append(send(x_out.at[:, cols], x_in.at[:, cols], px_ss.at[j], px_rs.at[j], {"tp": x_peer}))
        px[j].start()
    weights_on(0, 2)
    for j in range(2):
        pc[j, 1].wait_recv()
        px[j].wait_recv()
    projected = proj[row_block(t)].astype(f32) + core_in[1].astype(f32) + x_in[...].astype(f32)
    mid = (resid[...].astype(f32) + projected).astype(bf16)
    middle[...] = mid
    mid32 = mid.astype(f32)
    normed = mid32 * lax.rsqrt(jnp.mean(mid32 * mid32, axis=-1, keepdims=True) + NORM_EPS)
    act[pl.ds(s * rows + t * mine, mine)] = (normed * norm_gain[...].astype(f32)[None]).astype(bf16)

    half_mine = mine // 2
    ax, ac, az = {}, {}, {}

    def block(i, half, who):
        return act.at[pl.ds(planes[i] * rows + who * mine + half * half_mine, half_mine)]

    def spread(i, half):
        ref = block(i, half, t)
        ax[i, half] = send(ref, ref, ax_ss.at[i, half], ax_rs.at[i, half], {"tp": x_peer})
        ax[i, half].start()
        ac[i, half, 0] = send(ref, ref, ac_ss.at[i, half, 0], ac_rs.at[i, half, 0], {"tp": c_peer})
        ac[i, half, 0].start()

    def cross(i):
        for half in range(2):
            ax[i, half].wait_recv()
            ref = block(i, half, x_peer)
            ac[i, half, 1] = send(ref, ref, ac_ss.at[i, half, 1], ac_rs.at[i, half, 1], {"tp": c_peer})
            ac[i, half, 1].start()

    def onward(i):
        return ((planes[i] < s) & (s < sp_n - 1)) | ((planes[i] > s) & (s > 0))

    def next_hop(i, half):
        ref = block(i, half, t)
        to = jnp.where(planes[i] < s, s + 1, s - 1)
        to = jnp.clip(to, 0, sp_n - 1)
        return send(ref, ref, az_ss.at[i, half, 0], az_rs.at[planes[i], half], {"sp": to})

    def first_hop(half, way):
        ref = block(0, half, t)
        return send(ref, ref, az_ss.at[0, half, (1 - way) // 2], az_rs.at[s, half], {"sp": s + way})

    def ends(way):
        return (s < sp_n - 1) if way == 1 else (s > 0)

    def last_of(i, way):
        return (planes[i] == 0) & (s > 0) if way == 1 else (planes[i] == sp_n - 1) & (s < sp_n - 1)

    for half in range(2):
        for way in (1, -1):
            @pl.when(ends(way))
            def _():
                first_hop(half, way).start()
        spread(0, half)
    for way in (1, -1):
        @pl.when((s == 0) if way == 1 else (s == sp_n - 1))
        def _():
            weights_out(1, way)

    def gather(i):
        for half in range(2):
            ref = block(i, half, t)
            send(ref, ref, az_ss.at[i, half, 1], az_rs.at[planes[i], half], {"sp": planes[i]}).wait_recv()

            @pl.when(onward(i))
            def _():
                next_hop(i, half).start()
            spread(i, half)
        for way in (1, -1):
            @pl.when(last_of(i, way))
            def _():
                weights_out(1, way)

    def ready(i):
        for half in range(2):
            for k in range(2):
                ac[i, half, k].wait_recv()

    def lift(i):
        lifted = dot32(act[pl.ds(planes[i] * rows, rows)], up_full[...])
        hidden[i] = jnp.square(jnp.maximum(lifted, 0.0)).astype(bf16)

    rc, rx, rz = {}, {}, {}

    def lower(i, j):
        cols = cols_of(planes[j])
        part[i, :, cols] = dot32(hidden[i], down_full[:, cols]).astype(bf16)
        for k, who in enumerate((cx_peer, c_peer)):
            rc[i, j, k] = send(part.at[i, row_block(who), cols], core_recv.at[i, k, :, cols],
                               rc_ss.at[i, j, k], rc_rs.at[i, j, k], {"tp": c_peer})
            rc[i, j, k].start()

    def across(i, j):
        cols = cols_of(planes[j])
        rc[i, j, 0].wait_recv()
        x_send[i, :, cols] = (part[i, row_block(x_peer), cols].astype(f32)
                              + core_recv[i, 0, :, cols].astype(f32)).astype(bf16)
        rx[i, j] = send(x_send.at[i, :, cols], x_recv.at[i, :, cols], rx_ss.at[i, j], rx_rs.at[i, j], {"tp": x_peer})
        rx[i, j].start()

    def home(i, j):
        cols = cols_of(planes[j])
        rc[i, j, 1].wait_recv()
        rx[i, j].wait_recv()
        term = (part[i, row_block(t), cols].astype(f32) + core_recv[i, 1, :, cols].astype(f32)
                + x_recv[i, :, cols].astype(f32))
        if i == 0:
            total[:, cols] = term
            return
        z_send[i, :, cols] = term.astype(bf16)
        rz[i, j] = send(z_send.at[i, :, cols], z_recv.at[s, :, cols], rz_ss.at[i, j], rz_rs.at[s, planes[j]],
                        {"sp": planes[i]})
        rz[i, j].start()

    steps = []

    def run(i, j):
        lower(i, j)
        steps.append((i, j))
        if len(steps) > 1:
            across(*steps[-2])
        if len(steps) > 3:
            home(*steps[-4])

    weights_on(0, 3)
    for i in range(4, sp_n):
        weights_on(0, i)
    cross(0)
    gather(1)
    ready(0)
    for i in range(1, sp_n):
        weight_pass(0, i).wait_recv()
    lift(0)
    run(0, 0)
    for i in range(1, sp_n):
        cross(i)
        if i + 1 < sp_n:
            gather(i + 1)
        else:
            weights_on(1, 1)
        ready(i)
        lift(i)
        run(i, 0)
    for j in range(1, sp_n):
        weight_pass(1, j).wait_recv()
        if j + 1 < sp_n:
            weights_on(1, j + 1)
        for i in list(range(1, sp_n)) + [0]:
            run(i, j)
    across(*steps[-1])
    for step in steps[-3:]:
        home(*step)

    mixer = total[...]
    for i in range(1, sp_n):
        for j in range(sp_n):
            cols = cols_of(j)
            ref = z_recv.at[planes[i], :, cols]
            send(ref, ref, rz_ss.at[i, j], rz_rs.at[planes[i], j], {"sp": planes[i]}).wait_recv()
        mixer = mixer + z_recv[planes[i]].astype(f32)
    out[...] = (middle[...].astype(f32) + mixer).astype(bf16)

    for k in range(sp_n):
        for way in (1, -1):
            @pl.when(passes(k, way))
            def _():
                kv_pass(k, way).wait_send()
    for half in range(2):
        for way in (1, -1):
            @pl.when(ends(way))
            def _():
                first_hop(half, way).wait_send()
        for i in range(1, sp_n):
            @pl.when(onward(i))
            def _():
                next_hop(i, half).wait_send()
    for kind in range(2):
        for i in range(1, sp_n):
            weight_send(kind, i).wait_send()
            weight_pass(kind, i).wait_send()
    for group in (pc, ax, ac, rc, rx, rz):
        for copy in group.values():
            copy.wait_send()
    for copy in px:
        copy.wait_send()


def fused(sizes, resid_in, query_narrow, key_narrow, value_narrow, query_wide, key_wide, value_wide,
          lambda_narrow, lambda_wide, head_gain, out_narrow, out_wide, norm_gain, up_weight, down_weight):
    grp_n, sp_n, tp_n = sizes
    bf16, f32 = jnp.bfloat16, jnp.float32
    rows, v_width = query_narrow.shape[0], value_narrow.shape[2]
    spots, maps, flat = [], [], []
    kv_at = order = 0
    for query, key, value in ((query_narrow, key_narrow, value_narrow), (query_wide, key_wide, value_wide)):
        heads, both = query.shape[1:]
        kheads = key.shape[1]
        spots += [(kv_at, kheads * both), (kv_at + kheads * both, kheads * v_width)]
        flat += [key.reshape(rows, kheads * both), value.reshape(rows, kheads * v_width)]
        some = []
        for h in range(heads):
            kh = h // (heads // kheads)
            some.append((order, kh, both // 2, kv_at + kh * both, kv_at + kheads * both + kh * v_width))
            order += 1
        maps.append(some)
        kv_at += kheads * (both + v_width)
    mine, width = resid_in.shape
    deep, hid = up_weight.shape[0], up_weight.shape[1] // sp_n
    vm, sm, anyw = (pl.BlockSpec(memory_space=m) for m in (pltpu.VMEM, pltpu.SMEM, pl.ANY))
    dma = pltpu.SemaphoreType.DMA
    n = sp_n
    scratch = [
        pltpu.VMEM(query_narrow.shape, bf16),
        pltpu.VMEM(query_wide.shape, bf16),
        pltpu.VMEM((mine, width), bf16),
        pltpu.VMEM(out_narrow.shape, bf16),
        pltpu.VMEM(out_wide.shape, bf16),
        pltpu.VMEM((n * rows, kv_at), bf16),
        pltpu.VMEM((rows, order * v_width), bf16),
        pltpu.VMEM((rows, width), bf16),
        pltpu.VMEM((2, mine, width), bf16),
        pltpu.VMEM((mine, width), bf16),
        pltpu.VMEM((mine, width), bf16),
        pltpu.VMEM((mine, width), bf16),
        pltpu.VMEM((n * rows, width), bf16),
        pltpu.VMEM((n, rows, hid), bf16),
        pltpu.VMEM((width, hid), bf16),
        pltpu.VMEM((hid, width), bf16),
        pltpu.VMEM((n, rows, width), bf16),
        pltpu.VMEM((n, 2, mine, width), bf16),
        pltpu.VMEM((n, mine, width), bf16),
        pltpu.VMEM((n, mine, width), bf16),
        pltpu.VMEM((n, mine, width), bf16),
        pltpu.VMEM((n, mine, width), bf16),
        pltpu.VMEM((mine, width), f32),
        dma((11,)),
        *(dma(k) for k in ((2, n), (2, n), (2, n), (2, 2), (2,)) for _ in range(2)),
        dma((n, 2, 2)), dma((n, 2)),
        *(dma(k) for k in ((n, 2), (n, 2, 2), (n, n, 2), (n, n), (n, n)) for _ in range(2)),
    ]
    return pl.pallas_call(
        lambda *refs: layer_kernel((grp_n, sp_n, tp_n, tuple(spots), tuple(maps)), *refs),
        out_shape=jax.ShapeDtypeStruct(resid_in.shape, bf16),
        in_specs=[anyw] * 7 + [sm, sm, vm, anyw, anyw, vm, anyw, anyw],
        out_specs=vm,
        scratch_shapes=scratch,
        compiler_params=pltpu.CompilerParams(
            collective_id=0, has_side_effects=True, vmem_limit_bytes=VMEM_BYTES),
        name="layer",
    )(resid_in, query_narrow, flat[0], flat[1], query_wide, flat[2], flat[3], lambda_narrow, lambda_wide,
      head_gain, out_narrow, out_wide, norm_gain, up_weight, down_weight)


def fits(sizes, resid_in, query_narrow, query_wide, up_weight):
    grp_n, sp_n, tp_n = sizes
    rows, width = query_narrow.shape[0], resid_in.shape[1]
    held = 2 * width * (3 * sp_n * rows + 2 * rows + 2 * up_weight.shape[1] // sp_n)
    return (grp_n == 2 and tp_n == 4 and sp_n >= 4 and up_weight.shape[1] % (sp_n * 256) == 0
            and up_weight.shape[0] % 256 == 0 and resid_in.shape[0] % 32 == 0 and held < VMEM_BYTES // 2
            and query_narrow.shape[2] == 128 and query_wide.shape[2] % 256 == 0)


def solution(mesh):
    placed = (
        P(("grp", "sp", "tp"), None),
        P(("grp", "sp"), "tp", None),
        P(("grp", "sp"), "tp", None),
        P(("grp", "sp"), "tp", None),
        P(("grp", "sp"), "tp", None),
        P(("grp", "sp"), "tp", None),
        P(("grp", "sp"), "tp", None),
        P("tp"),
        P("tp"),
        P(),
        P("tp", None),
        P("tp", None),
        P(),
        P("sp", "tp"),
        P("tp", "sp"),
    )
    sizes = tuple(mesh.shape[axis] for axis in ("grp", "sp", "tp"))

    def layer(*blocks):
        if fits(sizes, blocks[0], blocks[1], blocks[4], blocks[13]):
            return fused(sizes, *blocks)
        return shards(*blocks)

    return jax.shard_map(
        layer, mesh=mesh, in_specs=placed, out_specs=P(("grp", "sp", "tp"), None), check_vma=False
    )
```

```python
import functools
import math

import jax
import jax.numpy as jnp
from jax import lax
from jax.experimental import pallas as pl
from jax.experimental.pallas import tpu as pltpu
from jax.sharding import PartitionSpec as P

NORM_EPS = 1e-06
OUT_SCALE = 0.8


def empty_state(query, key_head_stack, value_width):
    row_count, head_count = (query.shape[0], query.shape[1])
    group_size = head_count // key_head_stack
    row_top = jnp.full((key_head_stack, group_size, 2, row_count), -jnp.inf, jnp.float32)
    row_total = jnp.zeros((key_head_stack, group_size, 2, row_count), jnp.float32)
    weighted_values = jnp.zeros(
        (key_head_stack, group_size, 2, row_count, value_width), jnp.float32
    )
    return (row_top, row_total, weighted_values)


def absorb(states, query, key_rows, values):
    row_count, head_count = (query.shape[0], query.shape[1])
    key_head_stack = key_rows.shape[1]
    half_width = key_rows.shape[2] // 2
    group_size = head_count // key_head_stack
    value_width = values.shape[2]
    amount = key_rows.shape[0]
    block_rows = math.gcd(amount, 512)
    rotation_count = amount // block_rows
    grouped = query.reshape(row_count, key_head_stack, group_size, 2, half_width)
    key_block_list = key_rows.reshape(rotation_count, block_rows, key_head_stack, 2, half_width)
    value_blocks = values.reshape(rotation_count, block_rows, key_head_stack, value_width)

    def visit(running, kv_pair):
        row_top, row_total, weighted_values = running
        key_blk, value_blk = kv_pair
        scores = jnp.einsum(
            "tkgcd,skcd->kgcts", grouped, key_blk, preferred_element_type=jnp.float32
        ) * half_width ** (-0.5)
        new_top = jnp.maximum(row_top, jnp.max(scores, axis=-1))
        rescale = jnp.exp(row_top - new_top)
        powers = jnp.exp(scores - new_top[..., None])
        row_total = row_total * rescale + jnp.sum(powers, axis=-1)
        weighted_values = weighted_values * rescale[..., None] + jnp.einsum(
            "iodph,hie->iodpe",
            powers.astype(jnp.bfloat16),
            value_blk,
            preferred_element_type=jnp.float32,
        )
        return ((new_top, row_total, weighted_values), None)

    outcome, _ = lax.scan(visit, states, (key_block_list, value_blocks))
    return outcome


def finish(states, lambdas, gain_vec):
    row_top, row_total, weighted_values = states
    key_head_stack, group_size, row_count = (row_top.shape[0], row_top.shape[1], row_top.shape[3])
    value_width = weighted_values.shape[4]
    first_map = weighted_values[:, :, 0] / row_total[:, :, 0, :, None]
    second_map = weighted_values[:, :, 1] / row_total[:, :, 1, :, None]
    mixed = first_map - lambdas.reshape(key_head_stack, group_size)[:, :, None, None] * second_map
    normed = (
        mixed
        * lax.rsqrt(jnp.mean(mixed * mixed, axis=-1, keepdims=True) + NORM_EPS)
        * gain_vec
        * OUT_SCALE
    )
    normed = normed.astype(jnp.bfloat16).transpose(2, 0, 1, 3)
    return normed.reshape(row_count, key_head_stack * group_size * value_width)


def attend(
    query_narrow,
    key_narrow,
    value_narrow,
    query_wide,
    key_wide,
    value_wide,
    lambda_narrow,
    lambda_wide,
    head_gain,
):
    initial = (
        empty_state(query_narrow, key_narrow.shape[1], value_narrow.shape[2]),
        empty_state(query_wide, key_wide.shape[1], value_wide.shape[2]),
    )
    narrow_keys = lax.all_gather(key_narrow, "sp", axis=0, tiled=True)
    narrow_values = lax.all_gather(value_narrow, "sp", axis=0, tiled=True)
    wide_keys = lax.all_gather(key_wide, "sp", axis=0, tiled=True)
    wide_values = lax.all_gather(value_wide, "sp", axis=0, tiled=True)
    narrow_state = absorb(initial[0], query_narrow, narrow_keys, narrow_values)
    wide_state = absorb(initial[1], query_wide, wide_keys, wide_values)
    return (
        finish(narrow_state, lambda_narrow, head_gain),
        finish(wide_state, lambda_wide, head_gain),
    )


def shards(
    resid_in,
    query_narrow,
    key_narrow,
    value_narrow,
    query_wide,
    key_wide,
    value_wide,
    lambda_narrow,
    lambda_wide,
    head_gain,
    out_narrow,
    out_wide,
    norm_gain,
    up_weight,
    down_weight,
):
    att_narrow, att_wide = attend(
        query_narrow,
        key_narrow,
        value_narrow,
        query_wide,
        key_wide,
        value_wide,
        lambda_narrow,
        lambda_wide,
        head_gain,
    )
    projected = lax.psum_scatter(
        (
            jnp.dot(att_narrow, out_narrow, preferred_element_type=jnp.float32)
            + jnp.dot(att_wide, out_wide, preferred_element_type=jnp.float32)
        ).astype(jnp.bfloat16),
        "tp",
        scatter_dimension=0,
        tiled=True,
    ).astype(jnp.float32)
    middle = (resid_in.astype(jnp.float32) + projected).astype(jnp.bfloat16)
    middle_f32 = middle.astype(jnp.float32)
    normed = middle_f32 * lax.rsqrt(
        jnp.mean(middle_f32 * middle_f32, axis=-1, keepdims=True) + NORM_EPS
    )
    normed = (normed * norm_gain.astype(jnp.float32)).astype(jnp.bfloat16)
    whole_rows = lax.all_gather(normed, "tp", axis=0, tiled=True)
    up_collected = lax.all_gather(up_weight, "sp", axis=0, tiled=True)
    lifted = jnp.dot(whole_rows, up_collected, preferred_element_type=jnp.float32)
    activated = jnp.square(jax.nn.relu(lifted)).astype(jnp.bfloat16)
    partials = jnp.dot(
        activated,
        lax.all_gather(down_weight, "sp", axis=1, tiled=True),
        preferred_element_type=jnp.float32,
    )
    mixer_out = lax.psum_scatter(
        partials.astype(jnp.bfloat16), "tp", scatter_dimension=0, tiled=True
    ).astype(jnp.float32)
    return (middle_f32 + mixer_out).astype(jnp.bfloat16)


LOG2E = math.log2(math.e)
VMEM_BYTES = 60 * 2**20


def dot32(a, b):
    return jnp.dot(a, b, preferred_element_type=jnp.float32)


def layer_kernel(plan, resid_in, qn_in, kn_in, vn_in, qw_in, kw_in, vw_in, lam_n, lam_w, head_gain,
                 outn_in, outw_in, norm_gain, up, down,
                 out, qn, qw, queue, tops, totals, sums, resid, out_n, out_w, kv_full, att, proj, core_in, x_out, x_in, middle, act,
                 hidden, up_full, down_full, part, core_recv, x_send, x_recv, z_send, z_recv, total,
                 go, local, kv_ss, kv_rs, wz_ss, wz_rs, wy_ss, wy_rs, pc_ss, pc_rs, px_ss, px_rs,
                 az_ss, az_rs, ax_ss, ax_rs, ac_ss, ac_rs, rc_ss, rc_rs, rx_ss, rx_rs, rz_ss, rz_rs):
    grp_n, sp_n, tp_n, spots, maps = plan
    g, s, t = lax.axis_index("grp"), lax.axis_index("sp"), lax.axis_index("tp")
    rows = qn.shape[0]
    mine, width = resid.shape
    deep = up.shape[0]
    hid = up_full.shape[1]
    f32, bf16 = jnp.float32, jnp.bfloat16
    x_peer = lax.rem(t + 2, tp_n)
    c_peer = t + 1 - 2 * lax.rem(t, 2)
    cx_peer = lax.rem(c_peer + 2, tp_n)
    y_peer = 1 - g

    def by_distance(sign):
        lists = [sorted(range(sp_n), key=lambda p: (abs(p - me), sign * abs(2 * p + 1 - sp_n)))
                 for me in range(sp_n)]
        found = [s]
        for i in range(1, sp_n):
            at = lists[0][i]
            for me in range(1, sp_n):
                at = jnp.where(s == me, lists[me][i], at)
            found.append(at)
        return found

    planes, sources = by_distance(1), by_distance(-1)

    def send(src, dst, ss, rs, dev):
        return pltpu.make_async_remote_copy(
            src_ref=src, dst_ref=dst, send_sem=ss, recv_sem=rs,
            device_id=dev, device_id_type=pl.DeviceIdType.MESH)

    def cols_of(p):
        return pl.ds(pl.multiple_of(p * deep, 128), deep)

    loads = []

    def load(src, dst):
        copy = pltpu.make_async_copy(src, dst, local.at[len(loads)])
        copy.start()
        loads.append(copy)

    own = pl.ds(s * rows, rows)
    for ref, (at, size) in zip((kn_in, vn_in, kw_in, vw_in), spots):
        load(ref, kv_full.at[own, at:at + size])
    load(qn_in, qn)
    load(qw_in, qw)
    load(outn_in, out_n)
    load(outw_in, out_w)
    load(resid_in, resid)
    load(up.at[:, pl.ds(pl.multiple_of(s * hid, 128), hid)], up_full.at[pl.ds(s * deep, deep)])
    load(down.at[pl.ds(s * hid, hid)], down_full.at[:, cols_of(s)])

    barrier = pltpu.get_barrier_semaphore()
    peers = [{"sp": lax.rem(s + d, sp_n)} for d in range(1, sp_n)]
    peers += [{"sp": lax.rem(s + d, sp_n), "tp": c_peer} for d in range(1, sp_n)]
    peers += [{"tp": x_peer}, {"tp": c_peer}, {"grp": y_peer}]
    for peer in peers:
        pl.semaphore_signal(barrier, inc=1, device_id=peer, device_id_type=pl.DeviceIdType.MESH)
    for copy in loads[:4]:
        copy.wait()
    pl.semaphore_wait(barrier, len(peers))

    half_d, half_h = deep // grp_n, hid // grp_n

    def weight_send(kind, i):
        to = sources[i]
        if kind == 0:
            return send(up.at[pl.ds(g * half_d, half_d), pl.ds(pl.multiple_of(to * hid, 128), hid)],
                        up_full.at[pl.ds(s * deep + g * half_d, half_d)],
                        wz_ss.at[0, i], wz_rs.at[0, s], {"sp": to})
        return send(down.at[pl.ds(to * hid + g * half_h, half_h)],
                    down_full.at[pl.ds(g * half_h, half_h), cols_of(s)],
                    wz_ss.at[1, i], wz_rs.at[1, s], {"sp": to})

    def weight_ref(kind, i):
        at = sources[i]
        if kind == 0:
            return up_full.at[pl.ds(at * deep + g * half_d, half_d)]
        return down_full.at[pl.ds(g * half_h, half_h), cols_of(at)]

    def weight_pass(kind, i):
        ref = weight_ref(kind, i)
        return send(ref, ref, wy_ss.at[kind, i], wy_rs.at[kind, i], {"grp": y_peer})

    edge = (s == 0) | (s == sp_n - 1)
    middle_plane = jnp.logical_not(edge)

    def weights_on(kind, i):
        ref = weight_ref(kind, i)
        send(ref, ref, wz_ss.at[kind, i], wz_rs.at[kind, sources[i]], {"sp": sources[i]}).wait_recv()
        weight_pass(kind, i).start()

    def weights_when(kind, when, i):
        @pl.when(when)
        def _():
            weights_on(kind, i)

    def ends(way):
        return (s < sp_n - 1) if way == 1 else (s > 0)

    def onward(i):
        return ((planes[i] < s) & (s < sp_n - 1)) | ((planes[i] > s) & (s > 0))

    def after(i):
        return jnp.clip(jnp.where(planes[i] < s, s + 1, s - 1), 0, sp_n - 1)

    def invite(kind):
        for i in range(1, sp_n):
            for who in (t, c_peer):
                pl.semaphore_signal(go.at[kind, s], inc=1, device_id={"sp": sources[i], "tp": who},
                                    device_id_type=pl.DeviceIdType.MESH)

    def answer(kind, when, wait=True, start=True):
        for i in range(1, sp_n):
            ahead_of = edge if i == 1 else False

            @pl.when(when(sources[i]) & jnp.logical_not(ahead_of))
            def _():
                if wait:
                    pl.semaphore_wait(go.at[kind, sources[i]], 2)
                if start:
                    weight_send(kind, i).start()

    def ahead(kind):
        @pl.when(edge)
        def _():
            weight_send(kind, 1).start()

    def is_edge(p):
        return (p == 0) | (p == sp_n - 1)

    def near(p):
        return (p == s + 1) | (p == s - 1)

    def to_middle(p):
        return jnp.logical_not(is_edge(p))

    def to_near_edge(p):
        return is_edge(p) & middle_plane & near(p)

    def to_far_edge(p):
        return is_edge(p) & middle_plane & jnp.logical_not(near(p))

    def across_all(p):
        return is_edge(p) & edge

    def noted(kind):
        @pl.when(edge)
        def _():
            pl.semaphore_wait(go.at[kind, sources[1]], 2)

    def keys_of(p):
        return kv_full.at[pl.ds(p * rows, rows)]

    def kv_first(way):
        return send(keys_of(s), keys_of(s), kv_ss.at[0, (1 - way) // 2], kv_rs.at[s], {"sp": s + way})

    def kv_next(i):
        ref = keys_of(planes[i])
        return send(ref, ref, kv_ss.at[i, 0], kv_rs.at[planes[i]], {"sp": after(i)})

    def kv_get(i):
        ref = keys_of(planes[i])
        send(ref, ref, kv_ss.at[i, 1], kv_rs.at[planes[i]], {"sp": planes[i]}).wait_recv()

        @pl.when(onward(i))
        def _():
            kv_next(i).start()

    for way in (1, -1):
        @pl.when(ends(way))
        def _():
            kv_first(way).start()
    ahead(0)

    for copy in loads[4:6]:
        copy.wait()
    lane = lax.broadcasted_iota(jnp.int32, (rows, 128), 1)
    spot = 0
    for kind, ref in enumerate((qn, qw)):
        queries = ref[...].astype(f32)
        for h in range(len(maps[kind])):
            half = maps[kind][h][2]
            for c in range(2):
                if half < 128:
                    queue[spot] = jnp.where((lane // half) == c, queries[:, h, :], 0.0).astype(bf16)
                else:
                    queue[spot] = queries[:, h, c * half:(c + 1) * half].astype(bf16)
                spot += 1

    def attend(blocks, final):
        spot = 0
        work = []
        for kind in range(2):
            for h, (order, kh, half, k_at, v_at) in enumerate(maps[kind]):
                for c in range(2):
                    key_at = k_at + (c * half if half == 128 else 0)
                    scores = [lax.dot_general(
                        queue[spot], kv_full[pl.ds(p * rows, rows), key_at:key_at + 128],
                        (((1,), (1,)), ((), ())), preferred_element_type=f32) for p in blocks]
                    top = jnp.max(functools.reduce(jnp.maximum, scores), axis=-1, keepdims=True)
                    work.append((scores, top, half ** -0.5 * LOG2E, v_at))
                    spot += 1
        sides = []
        for spot, (scores, top, scale, v_at) in enumerate(work):
            if final:
                before = tops[spot]
                top = jnp.maximum(top, before)
            powers = [jnp.exp2((one - top) * scale) for one in scores]
            row_total = jnp.sum(functools.reduce(jnp.add, powers), axis=-1, keepdims=True)
            summed = functools.reduce(jnp.add, [
                dot32(one.astype(bf16), kv_full[pl.ds(p * rows, rows), v_at:v_at + head_gain.shape[0]])
                for p, one in zip(blocks, powers)])
            if final:
                fade = jnp.exp2((before - top) * scale)
                sides.append((summed + sums[spot] * fade) * (1.0 / (row_total + totals[spot] * fade)))
            else:
                tops[spot] = top
                totals[spot] = row_total
                sums[spot] = summed
        spot = 0
        for kind in range(2):
            for h, (order, *_) in enumerate(maps[kind] if final else ()):
                lam = (lam_n if kind == 0 else lam_w)[h]
                mixed = sides[2 * order] - lam * sides[2 * order + 1]
                v_width = mixed.shape[1]
                normed = (mixed * lax.rsqrt(jnp.mean(mixed * mixed, axis=-1, keepdims=True) + NORM_EPS)
                          * (head_gain[...][None] * OUT_SCALE))
                att[:, order * v_width:(order + 1) * v_width] = normed.astype(bf16)

    for i in range(1, sp_n - 1):
        kv_get(i)
    attend(planes[:sp_n - 1], False)
    noted(0)
    answer(0, lambda p: to_middle(p) & edge)
    kv_get(sp_n - 1)
    invite(0)
    attend(planes[sp_n - 1:], True)
    answer(0, lambda p: to_middle(p) & middle_plane)
    for copy in loads[6:]:
        copy.wait()

    cut = out_n.shape[0]
    chunk = math.gcd(width, 512)
    n_half = width // 2

    def row_block(who):
        return pl.ds(who * mine, mine)

    pc = {}
    for j in range(2):
        cols = slice(j * n_half, (j + 1) * n_half)
        for at in range(j * n_half, (j + 1) * n_half, chunk):
            some = slice(at, at + chunk)
            proj[:, some] = (dot32(att[:, :cut], out_n[:, some]) + dot32(att[:, cut:], out_w[:, some])).astype(bf16)
        for i, who in enumerate((cx_peer, c_peer)):
            pc[j, i] = send(proj.at[row_block(who), cols], core_in.at[i, :, cols],
                            pc_ss.at[j, i], pc_rs.at[j, i], {"tp": c_peer})
            pc[j, i].start()
    weights_when(0, middle_plane, 1)
    px = []
    for j in range(2):
        cols = slice(j * n_half, (j + 1) * n_half)
        pc[j, 0].wait_recv()
        x_out[:, cols] = (proj[row_block(x_peer), cols].astype(f32) + core_in[0, :, cols].astype(f32)).astype(bf16)
        px.append(send(x_out.at[:, cols], x_in.at[:, cols], px_ss.at[j], px_rs.at[j], {"tp": x_peer}))
        px[j].start()
    answer(0, to_near_edge)
    answer(0, across_all)
    for j in range(2):
        pc[j, 1].wait_recv()
        px[j].wait_recv()
    projected = proj[row_block(t)].astype(f32) + core_in[1].astype(f32) + x_in[...].astype(f32)
    mid = (resid[...].astype(f32) + projected).astype(bf16)
    middle[...] = mid
    mid32 = mid.astype(f32)
    normed = mid32 * lax.rsqrt(jnp.mean(mid32 * mid32, axis=-1, keepdims=True) + NORM_EPS)
    act[pl.ds(s * rows + t * mine, mine)] = (normed * norm_gain[...].astype(f32)[None]).astype(bf16)

    half_mine = mine // 2
    ax, ac, az = {}, {}, {}

    def block(i, half, who):
        return act.at[pl.ds(planes[i] * rows + who * mine + half * half_mine, half_mine)]

    def spread(i, half):
        ref = block(i, half, t)
        ax[i, half] = send(ref, ref, ax_ss.at[i, half], ax_rs.at[i, half], {"tp": x_peer})
        ax[i, half].start()
        ac[i, half, 0] = send(ref, ref, ac_ss.at[i, half, 0], ac_rs.at[i, half, 0], {"tp": c_peer})
        ac[i, half, 0].start()

    def cross(i):
        for half in range(2):
            ax[i, half].wait_recv()
            ref = block(i, half, x_peer)
            ac[i, half, 1] = send(ref, ref, ac_ss.at[i, half, 1], ac_rs.at[i, half, 1], {"tp": c_peer})
            ac[i, half, 1].start()

    def next_hop(i, half):
        ref = block(i, half, t)
        return send(ref, ref, az_ss.at[i, half, 0], az_rs.at[planes[i], half], {"sp": after(i)})

    def first_hop(half, way):
        ref = block(0, half, t)
        return send(ref, ref, az_ss.at[0, half, (1 - way) // 2], az_rs.at[s, half], {"sp": s + way})

    for half in range(2):
        for way in (1, -1):
            @pl.when(ends(way))
            def _():
                first_hop(half, way).start()
        spread(0, half)
    ahead(1)

    def gather(i):
        for half in range(2):
            ref = block(i, half, t)
            send(ref, ref, az_ss.at[i, half, 1], az_rs.at[planes[i], half], {"sp": planes[i]}).wait_recv()

            @pl.when(onward(i))
            def _():
                next_hop(i, half).start()
            spread(i, half)

    def ready(i):
        for half in range(2):
            for k in range(2):
                ac[i, half, k].wait_recv()

    def lift(i):
        lifted = dot32(act[pl.ds(planes[i] * rows, rows)], up_full[...])
        hidden[i] = jnp.square(jnp.maximum(lifted, 0.0)).astype(bf16)

    rc, rx, rz = {}, {}, {}

    def lower(i, j):
        cols = cols_of(sources[j])
        part[i, :, cols] = dot32(hidden[i], down_full[:, cols]).astype(bf16)
        for k, who in enumerate((cx_peer, c_peer)):
            rc[i, j, k] = send(part.at[i, row_block(who), cols], core_recv.at[i, k, :, cols],
                               rc_ss.at[i, j, k], rc_rs.at[i, j, k], {"tp": c_peer})
            rc[i, j, k].start()

    def across(i, j):
        cols = cols_of(sources[j])
        rc[i, j, 0].wait_recv()
        x_send[i, :, cols] = (part[i, row_block(x_peer), cols].astype(f32)
                              + core_recv[i, 0, :, cols].astype(f32)).astype(bf16)
        rx[i, j] = send(x_send.at[i, :, cols], x_recv.at[i, :, cols], rx_ss.at[i, j], rx_rs.at[i, j], {"tp": x_peer})
        rx[i, j].start()

    def home(i, j):
        cols = cols_of(sources[j])
        rc[i, j, 1].wait_recv()
        rx[i, j].wait_recv()
        term = (part[i, row_block(t), cols].astype(f32) + core_recv[i, 1, :, cols].astype(f32)
                + x_recv[i, :, cols].astype(f32))
        if i == 0:
            total[:, cols] = term
            return
        z_send[i, :, cols] = term.astype(bf16)
        rz[i, j] = send(z_send.at[i, :, cols], z_recv.at[s, :, cols], rz_ss.at[i, j], rz_rs.at[s, sources[j]],
                        {"sp": planes[i]})
        rz[i, j].start()

    steps = []

    def run(i, j):
        lower(i, j)
        steps.append((i, j))
        if len(steps) > 1:
            across(*steps[-2])
        if len(steps) > 3:
            home(*steps[-4])

    answer(0, to_far_edge)
    weights_when(0, edge, 1)
    gather(1)
    weights_on(0, 2)
    for i in range(2, sp_n - 1):
        gather(i)
    answer(1, to_middle, wait=False)
    for i in range(3, sp_n):
        weights_on(0, i)
    cross(0)
    cross(1)
    gather(sp_n - 1)
    answer(1, to_near_edge, wait=False)
    invite(1)
    ready(0)
    noted(1)
    answer(1, to_middle, start=False)
    for i in range(1, sp_n):
        weight_pass(0, i).wait_recv()
    lift(0)
    run(0, 0)
    weights_when(1, middle_plane, 1)
    for i in range(1, sp_n):
        if i > 1:
            cross(i)
        ready(i)
        lift(i)
        run(i, 0)
        if i == 1:
            answer(1, to_near_edge, start=False)
            answer(1, to_far_edge)
            weights_when(1, edge, 1)
        if i + 1 < sp_n:
            weights_when(1, middle_plane, i + 1)
    answer(1, across_all)
    for i in range(2, sp_n - 1):
        weights_when(1, edge, i)
    for j in range(1, sp_n):
        weight_pass(1, j).wait_recv()
        for i in list(range(1, sp_n)) + [0]:
            run(i, j)
            if j == 1 and i == 0:
                weights_when(1, edge, sp_n - 1)
    across(*steps[-1])
    for step in steps[-3:]:
        home(*step)

    mixer = total[...]
    for i in range(1, sp_n):
        for j in range(sp_n):
            cols = cols_of(j)
            ref = z_recv.at[planes[i], :, cols]
            send(ref, ref, rz_ss.at[i, j], rz_rs.at[planes[i], j], {"sp": planes[i]}).wait_recv()
        mixer = mixer + z_recv[planes[i]].astype(f32)
    out[...] = (middle[...].astype(f32) + mixer).astype(bf16)

    for way in (1, -1):
        @pl.when(ends(way))
        def _():
            kv_first(way).wait_send()
    for i in range(1, sp_n):
        @pl.when(onward(i))
        def _():
            kv_next(i).wait_send()
    for half in range(2):
        for way in (1, -1):
            @pl.when(ends(way))
            def _():
                first_hop(half, way).wait_send()
        for i in range(1, sp_n):
            @pl.when(onward(i))
            def _():
                next_hop(i, half).wait_send()
    for kind in range(2):
        for i in range(1, sp_n):
            weight_send(kind, i).wait_send()
            weight_pass(kind, i).wait_send()
    for group in (pc, ax, ac, rc, rx, rz):
        for copy in group.values():
            copy.wait_send()
    for copy in px:
        copy.wait_send()


def fused(sizes, resid_in, query_narrow, key_narrow, value_narrow, query_wide, key_wide, value_wide,
          lambda_narrow, lambda_wide, head_gain, out_narrow, out_wide, norm_gain, up_weight, down_weight):
    grp_n, sp_n, tp_n = sizes
    bf16, f32 = jnp.bfloat16, jnp.float32
    rows, v_width = query_narrow.shape[0], value_narrow.shape[2]
    spots, maps, flat = [], [], []
    kv_at = order = 0
    for query, key, value in ((query_narrow, key_narrow, value_narrow), (query_wide, key_wide, value_wide)):
        heads, both = query.shape[1:]
        kheads = key.shape[1]
        spots += [(kv_at, kheads * both), (kv_at + kheads * both, kheads * v_width)]
        flat += [key.reshape(rows, kheads * both), value.reshape(rows, kheads * v_width)]
        some = []
        for h in range(heads):
            kh = h // (heads // kheads)
            some.append((order, kh, both // 2, kv_at + kh * both, kv_at + kheads * both + kh * v_width))
            order += 1
        maps.append(some)
        kv_at += kheads * (both + v_width)
    mine, width = resid_in.shape
    deep, hid = up_weight.shape[0], up_weight.shape[1] // sp_n
    vm, sm, anyw = (pl.BlockSpec(memory_space=m) for m in (pltpu.VMEM, pltpu.SMEM, pl.ANY))
    dma = pltpu.SemaphoreType.DMA
    n = sp_n
    scratch = [
        pltpu.VMEM(query_narrow.shape, bf16),
        pltpu.VMEM(query_wide.shape, bf16),
        pltpu.VMEM((2 * order, rows, 128), bf16),
        pltpu.VMEM((2 * order, rows, 1), f32),
        pltpu.VMEM((2 * order, rows, 1), f32),
        pltpu.VMEM((2 * order, rows, v_width), f32),
        pltpu.VMEM((mine, width), bf16),
        pltpu.VMEM(out_narrow.shape, bf16),
        pltpu.VMEM(out_wide.shape, bf16),
        pltpu.VMEM((n * rows, kv_at), bf16),
        pltpu.VMEM((rows, order * v_width), bf16),
        pltpu.VMEM((rows, width), bf16),
        pltpu.VMEM((2, mine, width), bf16),
        pltpu.VMEM((mine, width), bf16),
        pltpu.VMEM((mine, width), bf16),
        pltpu.VMEM((mine, width), bf16),
        pltpu.VMEM((n * rows, width), bf16),
        pltpu.VMEM((n, rows, hid), bf16),
        pltpu.VMEM((width, hid), bf16),
        pltpu.VMEM((hid, width), bf16),
        pltpu.VMEM((n, rows, width), bf16),
        pltpu.VMEM((n, 2, mine, width), bf16),
        pltpu.VMEM((n, mine, width), bf16),
        pltpu.VMEM((n, mine, width), bf16),
        pltpu.VMEM((n, mine, width), bf16),
        pltpu.VMEM((n, mine, width), bf16),
        pltpu.VMEM((mine, width), f32),
        pltpu.SemaphoreType.REGULAR((2, n)),
        dma((11,)),
        dma((n, 2)), dma((n,)),
        *(dma(k) for k in ((2, n), (2, n), (2, 2), (2,)) for _ in range(2)),
        dma((n, 2, 2)), dma((n, 2)),
        *(dma(k) for k in ((n, 2), (n, 2, 2), (n, n, 2), (n, n), (n, n)) for _ in range(2)),
    ]
    return pl.pallas_call(
        lambda *refs: layer_kernel((grp_n, sp_n, tp_n, tuple(spots), tuple(maps)), *refs),
        out_shape=pltpu.VMEM(resid_in.shape, bf16),
        in_specs=[anyw] * 7 + [sm, sm, vm, anyw, anyw, vm, anyw, anyw],
        out_specs=vm,
        scratch_shapes=scratch,
        compiler_params=pltpu.CompilerParams(
            collective_id=0, has_side_effects=True, vmem_limit_bytes=VMEM_BYTES),
        name="layer",
    )(resid_in, query_narrow, flat[0], flat[1], query_wide, flat[2], flat[3], lambda_narrow, lambda_wide,
      head_gain, out_narrow, out_wide, norm_gain, up_weight, down_weight)


def fits(sizes, resid_in, query_narrow, query_wide, up_weight):
    grp_n, sp_n, tp_n = sizes
    rows, width = query_narrow.shape[0], resid_in.shape[1]
    held = 2 * width * (3 * sp_n * rows + 2 * rows + 2 * up_weight.shape[1] // sp_n)
    return (grp_n == 2 and tp_n == 4 and sp_n >= 4 and up_weight.shape[1] % (sp_n * 256) == 0
            and up_weight.shape[0] % 256 == 0 and resid_in.shape[0] % 32 == 0 and held < VMEM_BYTES // 2
            and query_narrow.shape[2] == 128 and query_wide.shape[2] == 256)


def solution(mesh):
    placed = (
        P(("grp", "sp", "tp"), None),
        P(("grp", "sp"), "tp", None),
        P(("grp", "sp"), "tp", None),
        P(("grp", "sp"), "tp", None),
        P(("grp", "sp"), "tp", None),
        P(("grp", "sp"), "tp", None),
        P(("grp", "sp"), "tp", None),
        P("tp"),
        P("tp"),
        P(),
        P("tp", None),
        P("tp", None),
        P(),
        P("sp", "tp"),
        P("tp", "sp"),
    )
    sizes = tuple(mesh.shape[axis] for axis in ("grp", "sp", "tp"))

    def layer(*blocks):
        if fits(sizes, blocks[0], blocks[1], blocks[4], blocks[13]):
            return fused(sizes, *blocks)
        return shards(*blocks)

    return jax.shard_map(
        layer, mesh=mesh, in_specs=placed, out_specs=P(("grp", "sp", "tp"), None), check_vma=False
    )
```

```python
import functools
import math

import jax
import jax.numpy as jnp
from jax import lax
from jax.experimental import pallas as pl
from jax.experimental.pallas import tpu as pltpu
from jax.sharding import PartitionSpec as P

NORM_EPS = 1e-06
OUT_SCALE = 0.8


def empty_state(query, key_head_stack, value_width):
    row_count, head_count = (query.shape[0], query.shape[1])
    group_size = head_count // key_head_stack
    row_top = jnp.full((key_head_stack, group_size, 2, row_count), -jnp.inf, jnp.float32)
    row_total = jnp.zeros((key_head_stack, group_size, 2, row_count), jnp.float32)
    weighted_values = jnp.zeros(
        (key_head_stack, group_size, 2, row_count, value_width), jnp.float32
    )
    return (row_top, row_total, weighted_values)


def absorb(states, query, key_rows, values):
    row_count, head_count = (query.shape[0], query.shape[1])
    key_head_stack = key_rows.shape[1]
    half_width = key_rows.shape[2] // 2
    group_size = head_count // key_head_stack
    value_width = values.shape[2]
    amount = key_rows.shape[0]
    block_rows = math.gcd(amount, 512)
    rotation_count = amount // block_rows
    grouped = query.reshape(row_count, key_head_stack, group_size, 2, half_width)
    key_block_list = key_rows.reshape(rotation_count, block_rows, key_head_stack, 2, half_width)
    value_blocks = values.reshape(rotation_count, block_rows, key_head_stack, value_width)

    def visit(running, kv_pair):
        row_top, row_total, weighted_values = running
        key_blk, value_blk = kv_pair
        scores = jnp.einsum(
            "tkgcd,skcd->kgcts", grouped, key_blk, preferred_element_type=jnp.float32
        ) * half_width ** (-0.5)
        new_top = jnp.maximum(row_top, jnp.max(scores, axis=-1))
        rescale = jnp.exp(row_top - new_top)
        powers = jnp.exp(scores - new_top[..., None])
        row_total = row_total * rescale + jnp.sum(powers, axis=-1)
        weighted_values = weighted_values * rescale[..., None] + jnp.einsum(
            "iodph,hie->iodpe",
            powers.astype(jnp.bfloat16),
            value_blk,
            preferred_element_type=jnp.float32,
        )
        return ((new_top, row_total, weighted_values), None)

    outcome, _ = lax.scan(visit, states, (key_block_list, value_blocks))
    return outcome


def finish(states, lambdas, gain_vec):
    row_top, row_total, weighted_values = states
    key_head_stack, group_size, row_count = (row_top.shape[0], row_top.shape[1], row_top.shape[3])
    value_width = weighted_values.shape[4]
    first_map = weighted_values[:, :, 0] / row_total[:, :, 0, :, None]
    second_map = weighted_values[:, :, 1] / row_total[:, :, 1, :, None]
    mixed = first_map - lambdas.reshape(key_head_stack, group_size)[:, :, None, None] * second_map
    normed = (
        mixed
        * lax.rsqrt(jnp.mean(mixed * mixed, axis=-1, keepdims=True) + NORM_EPS)
        * gain_vec
        * OUT_SCALE
    )
    normed = normed.astype(jnp.bfloat16).transpose(2, 0, 1, 3)
    return normed.reshape(row_count, key_head_stack * group_size * value_width)


def attend(
    query_narrow,
    key_narrow,
    value_narrow,
    query_wide,
    key_wide,
    value_wide,
    lambda_narrow,
    lambda_wide,
    head_gain,
):
    initial = (
        empty_state(query_narrow, key_narrow.shape[1], value_narrow.shape[2]),
        empty_state(query_wide, key_wide.shape[1], value_wide.shape[2]),
    )
    narrow_keys = lax.all_gather(key_narrow, "sp", axis=0, tiled=True)
    narrow_values = lax.all_gather(value_narrow, "sp", axis=0, tiled=True)
    wide_keys = lax.all_gather(key_wide, "sp", axis=0, tiled=True)
    wide_values = lax.all_gather(value_wide, "sp", axis=0, tiled=True)
    narrow_state = absorb(initial[0], query_narrow, narrow_keys, narrow_values)
    wide_state = absorb(initial[1], query_wide, wide_keys, wide_values)
    return (
        finish(narrow_state, lambda_narrow, head_gain),
        finish(wide_state, lambda_wide, head_gain),
    )


def shards(
    resid_in,
    query_narrow,
    key_narrow,
    value_narrow,
    query_wide,
    key_wide,
    value_wide,
    lambda_narrow,
    lambda_wide,
    head_gain,
    out_narrow,
    out_wide,
    norm_gain,
    up_weight,
    down_weight,
):
    att_narrow, att_wide = attend(
        query_narrow,
        key_narrow,
        value_narrow,
        query_wide,
        key_wide,
        value_wide,
        lambda_narrow,
        lambda_wide,
        head_gain,
    )
    projected = lax.psum_scatter(
        (
            jnp.dot(att_narrow, out_narrow, preferred_element_type=jnp.float32)
            + jnp.dot(att_wide, out_wide, preferred_element_type=jnp.float32)
        ).astype(jnp.bfloat16),
        "tp",
        scatter_dimension=0,
        tiled=True,
    ).astype(jnp.float32)
    middle = (resid_in.astype(jnp.float32) + projected).astype(jnp.bfloat16)
    middle_f32 = middle.astype(jnp.float32)
    normed = middle_f32 * lax.rsqrt(
        jnp.mean(middle_f32 * middle_f32, axis=-1, keepdims=True) + NORM_EPS
    )
    normed = (normed * norm_gain.astype(jnp.float32)).astype(jnp.bfloat16)
    whole_rows = lax.all_gather(normed, "tp", axis=0, tiled=True)
    up_collected = lax.all_gather(up_weight, "sp", axis=0, tiled=True)
    lifted = jnp.dot(whole_rows, up_collected, preferred_element_type=jnp.float32)
    activated = jnp.square(jax.nn.relu(lifted)).astype(jnp.bfloat16)
    partials = jnp.dot(
        activated,
        lax.all_gather(down_weight, "sp", axis=1, tiled=True),
        preferred_element_type=jnp.float32,
    )
    mixer_out = lax.psum_scatter(
        partials.astype(jnp.bfloat16), "tp", scatter_dimension=0, tiled=True
    ).astype(jnp.float32)
    return (middle_f32 + mixer_out).astype(jnp.bfloat16)


LOG2E = math.log2(math.e)
VMEM_BYTES = 60 * 2**20


def dot32(a, b):
    return jnp.dot(a, b, preferred_element_type=jnp.float32)


def layer_kernel(plan, resid_in, qn_in, kn_in, vn_in, qw_in, kw_in, vw_in, lam_n, lam_w, head_gain,
                 outn_in, outw_in, norm_gain, up, down,
                 out, qn, qw, queue, tops, totals, sums, resid, out_n, out_w, kv_full, att, proj, core_in, x_out, x_in, middle, act,
                 hidden, up_full, down_full, part, core_recv, x_send, x_recv, z_send, z_recv, total,
                 go, local, kv_ss, kv_rs, wz_ss, wz_rs, wy_ss, wy_rs, pc_ss, pc_rs, px_ss, px_rs,
                 az_ss, az_rs, ax_ss, ax_rs, ac_ss, ac_rs, rc_ss, rc_rs, rx_ss, rx_rs, rz_ss, rz_rs):
    grp_n, sp_n, tp_n, shares, spots, maps = plan
    g, s, t = lax.axis_index("grp"), lax.axis_index("sp"), lax.axis_index("tp")
    rows = qn.shape[0]
    mine, width = resid.shape
    deep = up.shape[0]
    f32, bf16 = jnp.float32, jnp.bfloat16
    x_peer = lax.rem(t + 2, tp_n)
    c_peer = t + 1 - 2 * lax.rem(t, 2)
    cx_peer = lax.rem(c_peer + 2, tp_n)
    y_peer = 1 - g

    def by_distance(sign):
        lists = [sorted(range(sp_n), key=lambda p: (abs(p - me), sign * abs(2 * p + 1 - sp_n)))
                 for me in range(sp_n)]
        found = [s]
        for i in range(1, sp_n):
            at = lists[0][i]
            for me in range(1, sp_n):
                at = jnp.where(s == me, lists[me][i], at)
            found.append(at)
        return found

    planes, sources = by_distance(1), by_distance(-1)

    def send(src, dst, ss, rs, dev):
        return pltpu.make_async_remote_copy(
            src_ref=src, dst_ref=dst, send_sem=ss, recv_sem=rs,
            device_id=dev, device_id_type=pl.DeviceIdType.MESH)

    def cols_of(p):
        return pl.ds(pl.multiple_of(p * deep, 128), deep)

    loads = []

    def load(src, dst):
        copy = pltpu.make_async_copy(src, dst, local.at[len(loads)])
        copy.start()
        loads.append(copy)

    own = pl.ds(s * rows, rows)
    for ref, (at, size) in zip((kn_in, vn_in, kw_in, vw_in), spots):
        load(ref, kv_full.at[own, at:at + size])
    load(qn_in, qn)
    load(qw_in, qw)
    load(outn_in, out_n)
    load(outw_in, out_w)
    load(resid_in, resid)
    edge = (s == 0) | (s == sp_n - 1)
    middle_plane = jnp.logical_not(edge)

    def typed(body, p=None):
        at_edge = edge if p is None else (p == 0) | (p == sp_n - 1)
        for when, size in ((at_edge, shares[0]), (jnp.logical_not(at_edge), shares[1])):
            @pl.when(when)
            def _():
                body(size)

    def first_unit(p):
        return pl.multiple_of(p * shares[1] - jnp.where(p > 0, shares[1] - shares[0], 0), 128)

    def own_weights(size):
        units = pl.ds(first_unit(s), size)
        return (pltpu.make_async_copy(up.at[:, units], up_full.at[pl.ds(s * deep, deep), :size], local.at[9]),
                pltpu.make_async_copy(down.at[units], down_full.at[:size, cols_of(s)], local.at[10]))

    @typed
    def _(size):
        for copy in own_weights(size):
            copy.start()


    barrier = pltpu.get_barrier_semaphore()
    peers = [{"sp": lax.rem(s + d, sp_n)} for d in range(1, sp_n)]
    peers += [{"sp": lax.rem(s + d, sp_n), "tp": c_peer} for d in range(1, sp_n)]
    peers += [{"tp": x_peer}, {"tp": c_peer}, {"grp": y_peer}]
    for peer in peers:
        pl.semaphore_signal(barrier, inc=1, device_id=peer, device_id_type=pl.DeviceIdType.MESH)
    for copy in loads[:4]:
        copy.wait()
    pl.semaphore_wait(barrier, len(peers))

    half_d = deep // grp_n

    def weight_send(kind, i, size):
        to = sources[i]
        if kind == 0:
            return send(up.at[pl.ds(g * half_d, half_d), pl.ds(first_unit(to), size)],
                        up_full.at[pl.ds(s * deep + g * half_d, half_d), :size],
                        wz_ss.at[0, i], wz_rs.at[0, s], {"sp": to})
        half_h = size // grp_n
        return send(down.at[pl.ds(first_unit(to) + g * half_h, half_h)],
                    down_full.at[pl.ds(g * half_h, half_h), cols_of(s)],
                    wz_ss.at[1, i], wz_rs.at[1, s], {"sp": to})

    def weight_ref(kind, i, size):
        at = sources[i]
        if kind == 0:
            return up_full.at[pl.ds(at * deep + g * half_d, half_d), :size]
        half_h = size // grp_n
        return down_full.at[pl.ds(g * half_h, half_h), cols_of(at)]

    def weight_pass(kind, i, size):
        ref = weight_ref(kind, i, size)
        return send(ref, ref, wy_ss.at[kind, i], wy_rs.at[kind, i], {"grp": y_peer})

    def weights_begin(kind, i):
        typed(lambda size: weight_send(kind, i, size).start(), sources[i])

    def weights_in(kind, i):
        typed(lambda size: weight_pass(kind, i, size).wait_recv())

    def weights_got(kind, i, size):
        ref = weight_ref(kind, i, size)
        send(ref, ref, wz_ss.at[kind, i], wz_rs.at[kind, sources[i]], {"sp": sources[i]}).wait_recv()
        weight_pass(kind, i, size).start()

    def weights_on(kind, i):
        typed(lambda size: weights_got(kind, i, size))

    def weights_when(kind, where, i):
        @pl.when((edge, middle_plane)[where])
        def _():
            weights_got(kind, i, shares[where])

    def ends(way):
        return (s < sp_n - 1) if way == 1 else (s > 0)

    def onward(i):
        return ((planes[i] < s) & (s < sp_n - 1)) | ((planes[i] > s) & (s > 0))

    def after(i):
        return jnp.clip(jnp.where(planes[i] < s, s + 1, s - 1), 0, sp_n - 1)

    def invite(kind):
        for i in range(1, sp_n):
            for who in (t, c_peer):
                pl.semaphore_signal(go.at[kind, s], inc=1, device_id={"sp": sources[i], "tp": who},
                                    device_id_type=pl.DeviceIdType.MESH)

    def answer(kind, when, wait=True, start=True):
        for i in range(1, sp_n):
            ahead_of = edge if i == 1 else False

            @pl.when(when(sources[i]) & jnp.logical_not(ahead_of))
            def _():
                if wait:
                    pl.semaphore_wait(go.at[kind, sources[i]], 2)
                if start:
                    weights_begin(kind, i)

    def ahead(kind):
        @pl.when(edge)
        def _():
            weights_begin(kind, 1)

    def is_edge(p):
        return (p == 0) | (p == sp_n - 1)

    def near(p):
        return (p == s + 1) | (p == s - 1)

    def to_middle(p):
        return jnp.logical_not(is_edge(p))

    def to_near_edge(p):
        return is_edge(p) & middle_plane & near(p)

    def to_far_edge(p):
        return is_edge(p) & middle_plane & jnp.logical_not(near(p))

    def across_all(p):
        return is_edge(p) & edge

    def noted(kind):
        @pl.when(edge)
        def _():
            pl.semaphore_wait(go.at[kind, sources[1]], 2)

    def keys_of(p):
        return kv_full.at[pl.ds(p * rows, rows)]

    def kv_first(way):
        return send(keys_of(s), keys_of(s), kv_ss.at[0, (1 - way) // 2], kv_rs.at[s], {"sp": s + way})

    def kv_next(i):
        ref = keys_of(planes[i])
        return send(ref, ref, kv_ss.at[i, 0], kv_rs.at[planes[i]], {"sp": after(i)})

    def kv_get(i):
        ref = keys_of(planes[i])
        send(ref, ref, kv_ss.at[i, 1], kv_rs.at[planes[i]], {"sp": planes[i]}).wait_recv()

        @pl.when(onward(i))
        def _():
            kv_next(i).start()

    for way in (1, -1):
        @pl.when(ends(way))
        def _():
            kv_first(way).start()
    ahead(0)

    for copy in loads[4:6]:
        copy.wait()
    lane = lax.broadcasted_iota(jnp.int32, (rows, 128), 1)
    spot = 0
    for kind, ref in enumerate((qn, qw)):
        queries = ref[...].astype(f32)
        for h in range(len(maps[kind])):
            half = maps[kind][h][2]
            for c in range(2):
                if half < 128:
                    queue[spot] = jnp.where((lane // half) == c, queries[:, h, :], 0.0).astype(bf16)
                else:
                    queue[spot] = queries[:, h, c * half:(c + 1) * half].astype(bf16)
                spot += 1

    def attend(blocks, final):
        spot = 0
        work = []
        for kind in range(2):
            for h, (order, kh, half, k_at, v_at) in enumerate(maps[kind]):
                for c in range(2):
                    key_at = k_at + (c * half if half == 128 else 0)
                    scores = [lax.dot_general(
                        queue[spot], kv_full[pl.ds(p * rows, rows), key_at:key_at + 128],
                        (((1,), (1,)), ((), ())), preferred_element_type=f32) for p in blocks]
                    top = jnp.max(functools.reduce(jnp.maximum, scores), axis=-1, keepdims=True)
                    work.append((scores, top, half ** -0.5 * LOG2E, v_at))
                    spot += 1
        sides = []
        for spot, (scores, top, scale, v_at) in enumerate(work):
            if final:
                before = tops[spot]
                top = jnp.maximum(top, before)
            powers = [jnp.exp2((one - top) * scale) for one in scores]
            row_total = jnp.sum(functools.reduce(jnp.add, powers), axis=-1, keepdims=True)
            summed = functools.reduce(jnp.add, [
                dot32(one.astype(bf16), kv_full[pl.ds(p * rows, rows), v_at:v_at + head_gain.shape[0]])
                for p, one in zip(blocks, powers)])
            if final:
                fade = jnp.exp2((before - top) * scale)
                sides.append((summed + sums[spot] * fade) * (1.0 / (row_total + totals[spot] * fade)))
            else:
                tops[spot] = top
                totals[spot] = row_total
                sums[spot] = summed
        spot = 0
        for kind in range(2):
            for h, (order, *_) in enumerate(maps[kind] if final else ()):
                lam = (lam_n if kind == 0 else lam_w)[h]
                mixed = sides[2 * order] - lam * sides[2 * order + 1]
                v_width = mixed.shape[1]
                normed = (mixed * lax.rsqrt(jnp.mean(mixed * mixed, axis=-1, keepdims=True) + NORM_EPS)
                          * (head_gain[...][None] * OUT_SCALE))
                att[:, order * v_width:(order + 1) * v_width] = normed.astype(bf16)

    for i in range(1, sp_n - 1):
        kv_get(i)
    attend(planes[:sp_n - 1], False)
    noted(0)
    answer(0, lambda p: to_middle(p) & edge)
    kv_get(sp_n - 1)
    invite(0)
    attend(planes[sp_n - 1:], True)
    answer(0, lambda p: to_middle(p) & middle_plane)
    for copy in loads[6:]:
        copy.wait()

    @typed
    def _(size):
        for copy in own_weights(size):
            copy.wait()


    cut = out_n.shape[0]
    chunk = math.gcd(width, 512)
    n_half = width // 2

    def row_block(who):
        return pl.ds(who * mine, mine)

    pc = {}
    for j in range(2):
        cols = slice(j * n_half, (j + 1) * n_half)
        for at in range(j * n_half, (j + 1) * n_half, chunk):
            some = slice(at, at + chunk)
            proj[:, some] = (dot32(att[:, :cut], out_n[:, some]) + dot32(att[:, cut:], out_w[:, some])).astype(bf16)
        for i, who in enumerate((cx_peer, c_peer)):
            pc[j, i] = send(proj.at[row_block(who), cols], core_in.at[i, :, cols],
                            pc_ss.at[j, i], pc_rs.at[j, i], {"tp": c_peer})
            pc[j, i].start()
    weights_when(0, 1, 1)
    px = []
    for j in range(2):
        cols = slice(j * n_half, (j + 1) * n_half)
        pc[j, 0].wait_recv()
        x_out[:, cols] = (proj[row_block(x_peer), cols].astype(f32) + core_in[0, :, cols].astype(f32)).astype(bf16)
        px.append(send(x_out.at[:, cols], x_in.at[:, cols], px_ss.at[j], px_rs.at[j], {"tp": x_peer}))
        px[j].start()
    answer(0, to_near_edge)
    answer(0, across_all)
    for j in range(2):
        pc[j, 1].wait_recv()
        px[j].wait_recv()
    projected = proj[row_block(t)].astype(f32) + core_in[1].astype(f32) + x_in[...].astype(f32)
    mid = (resid[...].astype(f32) + projected).astype(bf16)
    middle[...] = mid
    mid32 = mid.astype(f32)
    normed = mid32 * lax.rsqrt(jnp.mean(mid32 * mid32, axis=-1, keepdims=True) + NORM_EPS)
    act[pl.ds(s * rows + t * mine, mine)] = (normed * norm_gain[...].astype(f32)[None]).astype(bf16)

    half_mine = mine // 2
    ax, ac, az = {}, {}, {}

    def block(i, half, who):
        return act.at[pl.ds(planes[i] * rows + who * mine + half * half_mine, half_mine)]

    def spread(i, half):
        ref = block(i, half, t)
        ax[i, half] = send(ref, ref, ax_ss.at[i, half], ax_rs.at[i, half], {"tp": x_peer})
        ax[i, half].start()
        ac[i, half, 0] = send(ref, ref, ac_ss.at[i, half, 0], ac_rs.at[i, half, 0], {"tp": c_peer})
        ac[i, half, 0].start()

    def cross(i):
        for half in range(2):
            ax[i, half].wait_recv()
            ref = block(i, half, x_peer)
            ac[i, half, 1] = send(ref, ref, ac_ss.at[i, half, 1], ac_rs.at[i, half, 1], {"tp": c_peer})
            ac[i, half, 1].start()

    def next_hop(i, half):
        ref = block(i, half, t)
        return send(ref, ref, az_ss.at[i, half, 0], az_rs.at[planes[i], half], {"sp": after(i)})

    def first_hop(half, way):
        ref = block(0, half, t)
        return send(ref, ref, az_ss.at[0, half, (1 - way) // 2], az_rs.at[s, half], {"sp": s + way})

    for half in range(2):
        for way in (1, -1):
            @pl.when(ends(way))
            def _():
                first_hop(half, way).start()
        spread(0, half)
    ahead(1)

    def gather(i):
        for half in range(2):
            ref = block(i, half, t)
            send(ref, ref, az_ss.at[i, half, 1], az_rs.at[planes[i], half], {"sp": planes[i]}).wait_recv()

            @pl.when(onward(i))
            def _():
                next_hop(i, half).start()
            spread(i, half)

    def ready(i):
        for half in range(2):
            for k in range(2):
                ac[i, half, k].wait_recv()

    def lift(i):
        @typed
        def _(size):
            lifted = dot32(act[pl.ds(planes[i] * rows, rows)], up_full[:, :size])
            hidden[i, :, :size] = jnp.square(jnp.maximum(lifted, 0.0)).astype(bf16)

    rc, rx, rz = {}, {}, {}

    def lower(i, j):
        cols = cols_of(sources[j])

        @typed
        def _(size):
            part[i, :, cols] = dot32(hidden[i, :, :size], down_full[:size, cols]).astype(bf16)

        for k, who in enumerate((cx_peer, c_peer)):
            rc[i, j, k] = send(part.at[i, row_block(who), cols], core_recv.at[i, k, :, cols],
                               rc_ss.at[i, j, k], rc_rs.at[i, j, k], {"tp": c_peer})
            rc[i, j, k].start()

    def across(i, j):
        cols = cols_of(sources[j])
        rc[i, j, 0].wait_recv()
        x_send[i, :, cols] = (part[i, row_block(x_peer), cols].astype(f32)
                              + core_recv[i, 0, :, cols].astype(f32)).astype(bf16)
        rx[i, j] = send(x_send.at[i, :, cols], x_recv.at[i, :, cols], rx_ss.at[i, j], rx_rs.at[i, j], {"tp": x_peer})
        rx[i, j].start()

    def home(i, j):
        cols = cols_of(sources[j])
        rc[i, j, 1].wait_recv()
        rx[i, j].wait_recv()
        term = (part[i, row_block(t), cols].astype(f32) + core_recv[i, 1, :, cols].astype(f32)
                + x_recv[i, :, cols].astype(f32))
        if i == 0:
            total[:, cols] = term
            return
        z_send[i, :, cols] = term.astype(bf16)
        rz[i, j] = send(z_send.at[i, :, cols], z_recv.at[s, :, cols], rz_ss.at[i, j], rz_rs.at[s, sources[j]],
                        {"sp": planes[i]})
        rz[i, j].start()

    steps = []

    def run(i, j):
        lower(i, j)
        steps.append((i, j))
        if len(steps) > 1:
            across(*steps[-2])
        if len(steps) > 3:
            home(*steps[-4])

    answer(0, to_far_edge)
    weights_when(0, 0, 1)
    gather(1)
    weights_on(0, 2)
    for i in range(2, sp_n - 1):
        gather(i)
    answer(1, to_middle, wait=False)
    for i in range(3, sp_n):
        weights_on(0, i)
    cross(0)
    cross(1)
    gather(sp_n - 1)
    answer(1, to_near_edge, wait=False)
    invite(1)
    ready(0)
    noted(1)
    answer(1, to_middle, start=False)
    for i in range(1, sp_n):
        weights_in(0, i)
    lift(0)
    run(0, 0)
    weights_when(1, 1, 1)
    for i in range(1, sp_n):
        if i > 1:
            cross(i)
        ready(i)
        lift(i)
        run(i, 0)
        if i == 1:
            answer(1, to_near_edge, start=False)
            answer(1, to_far_edge)
            weights_when(1, 0, 1)
        if i + 1 < sp_n:
            weights_when(1, 1, i + 1)
    answer(1, across_all)
    for i in range(2, sp_n - 1):
        weights_when(1, 0, i)
    for j in range(1, sp_n):
        weights_in(1, j)
        for i in list(range(1, sp_n)) + [0]:
            run(i, j)
            if j == 1 and i == 0:
                weights_when(1, 0, sp_n - 1)
    across(*steps[-1])
    for step in steps[-3:]:
        home(*step)

    mixer = total[...]
    for i in range(1, sp_n):
        for j in range(sp_n):
            cols = cols_of(j)
            ref = z_recv.at[planes[i], :, cols]
            send(ref, ref, rz_ss.at[i, j], rz_rs.at[planes[i], j], {"sp": planes[i]}).wait_recv()
        mixer = mixer + z_recv[planes[i]].astype(f32)
    out[...] = (middle[...].astype(f32) + mixer).astype(bf16)

    for way in (1, -1):
        @pl.when(ends(way))
        def _():
            kv_first(way).wait_send()
    for i in range(1, sp_n):
        @pl.when(onward(i))
        def _():
            kv_next(i).wait_send()
    for half in range(2):
        for way in (1, -1):
            @pl.when(ends(way))
            def _():
                first_hop(half, way).wait_send()
        for i in range(1, sp_n):
            @pl.when(onward(i))
            def _():
                next_hop(i, half).wait_send()
    for kind in range(2):
        for i in range(1, sp_n):
            typed(lambda size: weight_send(kind, i, size).wait_send(), sources[i])
            typed(lambda size: weight_pass(kind, i, size).wait_send())
    for group in (pc, ax, ac, rc, rx, rz):
        for copy in group.values():
            copy.wait_send()
    for copy in px:
        copy.wait_send()


def shares_of(up_weight):
    half = up_weight.shape[1] // 2
    small = half * 3 // 8 // 128 * 128
    return small, half - small


def fused(sizes, resid_in, query_narrow, key_narrow, value_narrow, query_wide, key_wide, value_wide,
          lambda_narrow, lambda_wide, head_gain, out_narrow, out_wide, norm_gain, up_weight, down_weight):
    grp_n, sp_n, tp_n = sizes
    bf16, f32 = jnp.bfloat16, jnp.float32
    rows, v_width = query_narrow.shape[0], value_narrow.shape[2]
    spots, maps, flat = [], [], []
    kv_at = order = 0
    for query, key, value in ((query_narrow, key_narrow, value_narrow), (query_wide, key_wide, value_wide)):
        heads, both = query.shape[1:]
        kheads = key.shape[1]
        spots += [(kv_at, kheads * both), (kv_at + kheads * both, kheads * v_width)]
        flat += [key.reshape(rows, kheads * both), value.reshape(rows, kheads * v_width)]
        some = []
        for h in range(heads):
            kh = h // (heads // kheads)
            some.append((order, kh, both // 2, kv_at + kh * both, kv_at + kheads * both + kh * v_width))
            order += 1
        maps.append(some)
        kv_at += kheads * (both + v_width)
    mine, width = resid_in.shape
    deep, shares = up_weight.shape[0], shares_of(up_weight)
    hid = shares[1]
    vm, sm, anyw = (pl.BlockSpec(memory_space=m) for m in (pltpu.VMEM, pltpu.SMEM, pl.ANY))
    dma = pltpu.SemaphoreType.DMA
    n = sp_n
    scratch = [
        pltpu.VMEM(query_narrow.shape, bf16),
        pltpu.VMEM(query_wide.shape, bf16),
        pltpu.VMEM((2 * order, rows, 128), bf16),
        pltpu.VMEM((2 * order, rows, 1), f32),
        pltpu.VMEM((2 * order, rows, 1), f32),
        pltpu.VMEM((2 * order, rows, v_width), f32),
        pltpu.VMEM((mine, width), bf16),
        pltpu.VMEM(out_narrow.shape, bf16),
        pltpu.VMEM(out_wide.shape, bf16),
        pltpu.VMEM((n * rows, kv_at), bf16),
        pltpu.VMEM((rows, order * v_width), bf16),
        pltpu.VMEM((rows, width), bf16),
        pltpu.VMEM((2, mine, width), bf16),
        pltpu.VMEM((mine, width), bf16),
        pltpu.VMEM((mine, width), bf16),
        pltpu.VMEM((mine, width), bf16),
        pltpu.VMEM((n * rows, width), bf16),
        pltpu.VMEM((n, rows, hid), bf16),
        pltpu.VMEM((width, hid), bf16),
        pltpu.VMEM((hid, width), bf16),
        pltpu.VMEM((n, rows, width), bf16),
        pltpu.VMEM((n, 2, mine, width), bf16),
        pltpu.VMEM((n, mine, width), bf16),
        pltpu.VMEM((n, mine, width), bf16),
        pltpu.VMEM((n, mine, width), bf16),
        pltpu.VMEM((n, mine, width), bf16),
        pltpu.VMEM((mine, width), f32),
        pltpu.SemaphoreType.REGULAR((2, n)),
        dma((11,)),
        dma((n, 2)), dma((n,)),
        *(dma(k) for k in ((2, n), (2, n), (2, 2), (2,)) for _ in range(2)),
        dma((n, 2, 2)), dma((n, 2)),
        *(dma(k) for k in ((n, 2), (n, 2, 2), (n, n, 2), (n, n), (n, n)) for _ in range(2)),
    ]
    return pl.pallas_call(
        lambda *refs: layer_kernel((grp_n, sp_n, tp_n, shares, tuple(spots), tuple(maps)), *refs),
        out_shape=pltpu.VMEM(resid_in.shape, bf16),
        in_specs=[anyw] * 7 + [sm, sm, vm, anyw, anyw, vm, anyw, anyw],
        out_specs=vm,
        scratch_shapes=scratch,
        compiler_params=pltpu.CompilerParams(
            collective_id=0, has_side_effects=True, vmem_limit_bytes=VMEM_BYTES),
        name="layer",
    )(resid_in, query_narrow, flat[0], flat[1], query_wide, flat[2], flat[3], lambda_narrow, lambda_wide,
      head_gain, out_narrow, out_wide, norm_gain, up_weight, down_weight)


def fits(sizes, resid_in, query_narrow, query_wide, up_weight):
    grp_n, sp_n, tp_n = sizes
    rows, width = query_narrow.shape[0], resid_in.shape[1]
    held = 2 * width * (3 * sp_n * rows + 2 * rows + 2 * up_weight.shape[1] // sp_n)
    return (grp_n == 2 and tp_n == 4 and sp_n == 4 and up_weight.shape[1] % 1024 == 0
            and up_weight.shape[0] % 256 == 0 and resid_in.shape[0] % 32 == 0 and held < VMEM_BYTES // 2
            and query_narrow.shape[2] == 128 and query_wide.shape[2] == 256)


def solution(mesh):
    placed = (
        P(("grp", "sp", "tp"), None),
        P(("grp", "sp"), "tp", None),
        P(("grp", "sp"), "tp", None),
        P(("grp", "sp"), "tp", None),
        P(("grp", "sp"), "tp", None),
        P(("grp", "sp"), "tp", None),
        P(("grp", "sp"), "tp", None),
        P("tp"),
        P("tp"),
        P(),
        P("tp", None),
        P("tp", None),
        P(),
        P("sp", "tp"),
        P("tp", "sp"),
    )
    sizes = tuple(mesh.shape[axis] for axis in ("grp", "sp", "tp"))

    def layer(*blocks):
        if fits(sizes, blocks[0], blocks[1], blocks[4], blocks[13]):
            return fused(sizes, *blocks)
        return shards(*blocks)

    return jax.shard_map(
        layer, mesh=mesh, in_specs=placed, out_specs=P(("grp", "sp", "tp"), None), check_vma=False
    )
```

```python
import functools
import math

import jax
import jax.numpy as jnp
from jax import lax
from jax.experimental import pallas as pl
from jax.experimental.pallas import tpu as pltpu
from jax.sharding import PartitionSpec as P

NORM_EPS = 1e-06
OUT_SCALE = 0.8


def empty_state(query, key_head_stack, value_width):
    row_count, head_count = (query.shape[0], query.shape[1])
    group_size = head_count // key_head_stack
    row_top = jnp.full((key_head_stack, group_size, 2, row_count), -jnp.inf, jnp.float32)
    row_total = jnp.zeros((key_head_stack, group_size, 2, row_count), jnp.float32)
    weighted_values = jnp.zeros(
        (key_head_stack, group_size, 2, row_count, value_width), jnp.float32
    )
    return (row_top, row_total, weighted_values)


def absorb(states, query, key_rows, values):
    row_count, head_count = (query.shape[0], query.shape[1])
    key_head_stack = key_rows.shape[1]
    half_width = key_rows.shape[2] // 2
    group_size = head_count // key_head_stack
    value_width = values.shape[2]
    amount = key_rows.shape[0]
    block_rows = math.gcd(amount, 512)
    rotation_count = amount // block_rows
    grouped = query.reshape(row_count, key_head_stack, group_size, 2, half_width)
    key_block_list = key_rows.reshape(rotation_count, block_rows, key_head_stack, 2, half_width)
    value_blocks = values.reshape(rotation_count, block_rows, key_head_stack, value_width)

    def visit(running, kv_pair):
        row_top, row_total, weighted_values = running
        key_blk, value_blk = kv_pair
        scores = jnp.einsum(
            "tkgcd,skcd->kgcts", grouped, key_blk, preferred_element_type=jnp.float32
        ) * half_width ** (-0.5)
        new_top = jnp.maximum(row_top, jnp.max(scores, axis=-1))
        rescale = jnp.exp(row_top - new_top)
        powers = jnp.exp(scores - new_top[..., None])
        row_total = row_total * rescale + jnp.sum(powers, axis=-1)
        weighted_values = weighted_values * rescale[..., None] + jnp.einsum(
            "iodph,hie->iodpe",
            powers.astype(jnp.bfloat16),
            value_blk,
            preferred_element_type=jnp.float32,
        )
        return ((new_top, row_total, weighted_values), None)

    outcome, _ = lax.scan(visit, states, (key_block_list, value_blocks))
    return outcome


def finish(states, lambdas, gain_vec):
    row_top, row_total, weighted_values = states
    key_head_stack, group_size, row_count = (row_top.shape[0], row_top.shape[1], row_top.shape[3])
    value_width = weighted_values.shape[4]
    first_map = weighted_values[:, :, 0] / row_total[:, :, 0, :, None]
    second_map = weighted_values[:, :, 1] / row_total[:, :, 1, :, None]
    mixed = first_map - lambdas.reshape(key_head_stack, group_size)[:, :, None, None] * second_map
    normed = (
        mixed
        * lax.rsqrt(jnp.mean(mixed * mixed, axis=-1, keepdims=True) + NORM_EPS)
        * gain_vec
        * OUT_SCALE
    )
    normed = normed.astype(jnp.bfloat16).transpose(2, 0, 1, 3)
    return normed.reshape(row_count, key_head_stack * group_size * value_width)


def attend(
    query_narrow,
    key_narrow,
    value_narrow,
    query_wide,
    key_wide,
    value_wide,
    lambda_narrow,
    lambda_wide,
    head_gain,
):
    initial = (
        empty_state(query_narrow, key_narrow.shape[1], value_narrow.shape[2]),
        empty_state(query_wide, key_wide.shape[1], value_wide.shape[2]),
    )
    narrow_keys = lax.all_gather(key_narrow, "sp", axis=0, tiled=True)
    narrow_values = lax.all_gather(value_narrow, "sp", axis=0, tiled=True)
    wide_keys = lax.all_gather(key_wide, "sp", axis=0, tiled=True)
    wide_values = lax.all_gather(value_wide, "sp", axis=0, tiled=True)
    narrow_state = absorb(initial[0], query_narrow, narrow_keys, narrow_values)
    wide_state = absorb(initial[1], query_wide, wide_keys, wide_values)
    return (
        finish(narrow_state, lambda_narrow, head_gain),
        finish(wide_state, lambda_wide, head_gain),
    )


def shards(
    resid_in,
    query_narrow,
    key_narrow,
    value_narrow,
    query_wide,
    key_wide,
    value_wide,
    lambda_narrow,
    lambda_wide,
    head_gain,
    out_narrow,
    out_wide,
    norm_gain,
    up_weight,
    down_weight,
):
    att_narrow, att_wide = attend(
        query_narrow,
        key_narrow,
        value_narrow,
        query_wide,
        key_wide,
        value_wide,
        lambda_narrow,
        lambda_wide,
        head_gain,
    )
    projected = lax.psum_scatter(
        (
            jnp.dot(att_narrow, out_narrow, preferred_element_type=jnp.float32)
            + jnp.dot(att_wide, out_wide, preferred_element_type=jnp.float32)
        ).astype(jnp.bfloat16),
        "tp",
        scatter_dimension=0,
        tiled=True,
    ).astype(jnp.float32)
    middle = (resid_in.astype(jnp.float32) + projected).astype(jnp.bfloat16)
    middle_f32 = middle.astype(jnp.float32)
    normed = middle_f32 * lax.rsqrt(
        jnp.mean(middle_f32 * middle_f32, axis=-1, keepdims=True) + NORM_EPS
    )
    normed = (normed * norm_gain.astype(jnp.float32)).astype(jnp.bfloat16)
    whole_rows = lax.all_gather(normed, "tp", axis=0, tiled=True)
    up_collected = lax.all_gather(up_weight, "sp", axis=0, tiled=True)
    lifted = jnp.dot(whole_rows, up_collected, preferred_element_type=jnp.float32)
    activated = jnp.square(jax.nn.relu(lifted)).astype(jnp.bfloat16)
    partials = jnp.dot(
        activated,
        lax.all_gather(down_weight, "sp", axis=1, tiled=True),
        preferred_element_type=jnp.float32,
    )
    mixer_out = lax.psum_scatter(
        partials.astype(jnp.bfloat16), "tp", scatter_dimension=0, tiled=True
    ).astype(jnp.float32)
    return (middle_f32 + mixer_out).astype(jnp.bfloat16)


LOG2E = math.log2(math.e)
VMEM_BYTES = 60 * 2**20


def dot32(a, b):
    return jnp.dot(a, b, preferred_element_type=jnp.float32)


def layer_kernel(plan, resid_in, qn_in, kn_in, vn_in, qw_in, kw_in, vw_in, lam_n, lam_w, head_gain,
                 outn_in, outw_in, norm_gain, up, down,
                 out, qn, qw, queue, tops, totals, sums, resid, out_n, out_w, kv_full, att, proj, core_in, x_out, x_in, middle, act,
                 hidden, up_full, down_full, part, core_recv, x_send, x_recv, z_send, z_recv, total,
                 go, local, kv_ss, kv_rs, wz_ss, wz_rs, wy_ss, wy_rs, pc_ss, pc_rs, px_ss, px_rs,
                 az_ss, az_rs, ax_ss, ax_rs, ac_ss, ac_rs, rc_ss, rc_rs, rx_ss, rx_rs, rz_ss, rz_rs):
    grp_n, sp_n, tp_n, shares, spots, maps = plan
    g, s, t = lax.axis_index("grp"), lax.axis_index("sp"), lax.axis_index("tp")
    rows = qn.shape[0]
    mine, width = resid.shape
    deep = up.shape[0]
    f32, bf16 = jnp.float32, jnp.bfloat16
    x_peer = lax.rem(t + 2, tp_n)
    c_peer = t + 1 - 2 * lax.rem(t, 2)
    cx_peer = lax.rem(c_peer + 2, tp_n)
    y_peer = 1 - g

    def by_distance(sign):
        lists = [sorted(range(sp_n), key=lambda p: (abs(p - me), sign * abs(2 * p + 1 - sp_n)))
                 for me in range(sp_n)]
        found = [s]
        for i in range(1, sp_n):
            at = lists[0][i]
            for me in range(1, sp_n):
                at = jnp.where(s == me, lists[me][i], at)
            found.append(at)
        return found

    planes, sources = by_distance(1), by_distance(-1)

    def send(src, dst, ss, rs, dev):
        return pltpu.make_async_remote_copy(
            src_ref=src, dst_ref=dst, send_sem=ss, recv_sem=rs,
            device_id=dev, device_id_type=pl.DeviceIdType.MESH)

    def cols_of(p):
        return pl.ds(pl.multiple_of(p * deep, 128), deep)

    loads = []

    def load(src, dst):
        copy = pltpu.make_async_copy(src, dst, local.at[len(loads)])
        copy.start()
        loads.append(copy)

    own = pl.ds(s * rows, rows)
    for ref, (at, size) in zip((kn_in, vn_in, kw_in, vw_in), spots):
        load(ref, kv_full.at[own, at:at + size])
    load(qn_in, qn)
    load(qw_in, qw)
    load(outn_in, out_n)
    load(outw_in, out_w)
    load(resid_in, resid)
    edge = (s == 0) | (s == sp_n - 1)
    middle_plane = jnp.logical_not(edge)

    def typed(body, p=None):
        at_edge = edge if p is None else (p == 0) | (p == sp_n - 1)
        for when, size in ((at_edge, shares[0]), (jnp.logical_not(at_edge), shares[1])):
            @pl.when(when)
            def _():
                body(size)

    def first_unit(p):
        return pl.multiple_of(p * shares[1] - jnp.where(p > 0, shares[1] - shares[0], 0), 128)

    def own_weights(size):
        units = pl.ds(first_unit(s), size)
        return (pltpu.make_async_copy(up.at[:, units], up_full.at[pl.ds(s * deep, deep), :size], local.at[9]),
                pltpu.make_async_copy(down.at[units], down_full.at[:size, cols_of(s)], local.at[10]))

    @typed
    def _(size):
        for copy in own_weights(size):
            copy.start()


    barrier = pltpu.get_barrier_semaphore()
    peers = [{"sp": lax.rem(s + d, sp_n)} for d in range(1, sp_n)]
    peers += [{"sp": lax.rem(s + d, sp_n), "tp": c_peer} for d in range(1, sp_n)]
    peers += [{"tp": x_peer}, {"tp": c_peer}, {"grp": y_peer}]
    for peer in peers:
        pl.semaphore_signal(barrier, inc=1, device_id=peer, device_id_type=pl.DeviceIdType.MESH)
    for copy in loads[:4]:
        copy.wait()
    pl.semaphore_wait(barrier, len(peers))

    half_d = deep // grp_n

    def weight_send(kind, i, size):
        to = sources[i]
        if kind == 0:
            return send(up.at[pl.ds(g * half_d, half_d), pl.ds(first_unit(to), size)],
                        up_full.at[pl.ds(s * deep + g * half_d, half_d), :size],
                        wz_ss.at[0, i], wz_rs.at[0, s], {"sp": to})
        half_h = size // grp_n
        return send(down.at[pl.ds(first_unit(to) + g * half_h, half_h)],
                    down_full.at[pl.ds(g * half_h, half_h), cols_of(s)],
                    wz_ss.at[1, i], wz_rs.at[1, s], {"sp": to})

    def weight_ref(kind, i, size):
        at = sources[i]
        if kind == 0:
            return up_full.at[pl.ds(at * deep + g * half_d, half_d), :size]
        half_h = size // grp_n
        return down_full.at[pl.ds(g * half_h, half_h), cols_of(at)]

    def weight_pass(kind, i, size):
        ref = weight_ref(kind, i, size)
        return send(ref, ref, wy_ss.at[kind, i], wy_rs.at[kind, i], {"grp": y_peer})

    def weights_begin(kind, i):
        typed(lambda size: weight_send(kind, i, size).start(), sources[i])

    def weights_in(kind, i):
        typed(lambda size: weight_pass(kind, i, size).wait_recv())

    def weights_got(kind, i, size):
        ref = weight_ref(kind, i, size)
        send(ref, ref, wz_ss.at[kind, i], wz_rs.at[kind, sources[i]], {"sp": sources[i]}).wait_recv()
        weight_pass(kind, i, size).start()

    def weights_on(kind, i):
        typed(lambda size: weights_got(kind, i, size))

    def weights_when(kind, where, i):
        @pl.when((edge, middle_plane)[where])
        def _():
            weights_got(kind, i, shares[where])

    def ends(way):
        return (s < sp_n - 1) if way == 1 else (s > 0)

    def onward(i):
        return ((planes[i] < s) & (s < sp_n - 1)) | ((planes[i] > s) & (s > 0))

    def after(i):
        return jnp.clip(jnp.where(planes[i] < s, s + 1, s - 1), 0, sp_n - 1)

    def invite(kind):
        for i in range(1, sp_n):
            for who in (t, c_peer):
                pl.semaphore_signal(go.at[kind, s], inc=1, device_id={"sp": sources[i], "tp": who},
                                    device_id_type=pl.DeviceIdType.MESH)

    def answer(kind, when, wait=True, start=True):
        for i in range(1, sp_n):
            ahead_of = edge if i == 1 else False

            @pl.when(when(sources[i]) & jnp.logical_not(ahead_of))
            def _():
                if wait:
                    pl.semaphore_wait(go.at[kind, sources[i]], 2)
                if start:
                    weights_begin(kind, i)

    def ahead(kind):
        @pl.when(edge)
        def _():
            weights_begin(kind, 1)

    def is_edge(p):
        return (p == 0) | (p == sp_n - 1)

    def near(p):
        return (p == s + 1) | (p == s - 1)

    def to_middle(p):
        return jnp.logical_not(is_edge(p))

    def to_near_edge(p):
        return is_edge(p) & middle_plane & near(p)

    def to_far_edge(p):
        return is_edge(p) & middle_plane & jnp.logical_not(near(p))

    def across_all(p):
        return is_edge(p) & edge

    def noted(kind):
        @pl.when(edge)
        def _():
            pl.semaphore_wait(go.at[kind, sources[1]], 2)

    def keys_of(p):
        return kv_full.at[pl.ds(p * rows, rows)]

    def kv_first(way):
        return send(keys_of(s), keys_of(s), kv_ss.at[0, (1 - way) // 2], kv_rs.at[s], {"sp": s + way})

    def kv_next(i):
        ref = keys_of(planes[i])
        return send(ref, ref, kv_ss.at[i, 0], kv_rs.at[planes[i]], {"sp": after(i)})

    def kv_get(i):
        ref = keys_of(planes[i])
        send(ref, ref, kv_ss.at[i, 1], kv_rs.at[planes[i]], {"sp": planes[i]}).wait_recv()

        @pl.when(onward(i))
        def _():
            kv_next(i).start()

    for way in (1, -1):
        @pl.when(ends(way))
        def _():
            kv_first(way).start()
    ahead(0)

    for copy in loads[4:6]:
        copy.wait()
    lane = lax.broadcasted_iota(jnp.int32, (rows, 128), 1)
    spot = 0
    for kind, ref in enumerate((qn, qw)):
        queries = ref[...].astype(f32)
        for h in range(len(maps[kind])):
            half = maps[kind][h][2]
            for c in range(2):
                if half < 128:
                    queue[spot] = jnp.where((lane // half) == c, queries[:, h, :], 0.0).astype(bf16)
                else:
                    queue[spot] = queries[:, h, c * half:(c + 1) * half].astype(bf16)
                spot += 1

    def attend(blocks, final):
        spot = 0
        work = []
        for kind in range(2):
            for h, (order, kh, half, k_at, v_at) in enumerate(maps[kind]):
                for c in range(2):
                    key_at = k_at + (c * half if half == 128 else 0)
                    scores = [lax.dot_general(
                        queue[spot], kv_full[pl.ds(p * rows, rows), key_at:key_at + 128],
                        (((1,), (1,)), ((), ())), preferred_element_type=f32) for p in blocks]
                    top = jnp.max(functools.reduce(jnp.maximum, scores), axis=-1, keepdims=True)
                    work.append((scores, top, half ** -0.5 * LOG2E, v_at))
                    spot += 1
        sides = []
        for spot, (scores, top, scale, v_at) in enumerate(work):
            if final:
                before = tops[spot]
                top = jnp.maximum(top, before)
            powers = [jnp.exp2((one - top) * scale) for one in scores]
            row_total = jnp.sum(functools.reduce(jnp.add, powers), axis=-1, keepdims=True)
            summed = functools.reduce(jnp.add, [
                dot32(one.astype(bf16), kv_full[pl.ds(p * rows, rows), v_at:v_at + head_gain.shape[0]])
                for p, one in zip(blocks, powers)])
            if final:
                fade = jnp.exp2((before - top) * scale)
                sides.append((summed + sums[spot] * fade) * (1.0 / (row_total + totals[spot] * fade)))
            else:
                tops[spot] = top
                totals[spot] = row_total
                sums[spot] = summed
        spot = 0
        for kind in range(2):
            for h, (order, *_) in enumerate(maps[kind] if final else ()):
                lam = (lam_n if kind == 0 else lam_w)[h]
                mixed = sides[2 * order] - lam * sides[2 * order + 1]
                v_width = mixed.shape[1]
                normed = (mixed * lax.rsqrt(jnp.mean(mixed * mixed, axis=-1, keepdims=True) + NORM_EPS)
                          * (head_gain[...][None] * OUT_SCALE))
                att[:, order * v_width:(order + 1) * v_width] = normed.astype(bf16)

    for i in range(1, sp_n - 1):
        kv_get(i)
    attend(planes[:sp_n - 1], False)
    noted(0)
    answer(0, lambda p: to_middle(p) & edge)
    kv_get(sp_n - 1)
    invite(0)
    answer(0, lambda p: to_middle(p) & middle_plane, wait=False)
    attend(planes[sp_n - 1:], True)
    answer(0, lambda p: to_middle(p) & middle_plane, start=False)
    for copy in loads[6:]:
        copy.wait()

    @typed
    def _(size):
        for copy in own_weights(size):
            copy.wait()


    cut = out_n.shape[0]
    chunk = math.gcd(width, 512)
    n_half = width // 2

    def row_block(who):
        return pl.ds(who * mine, mine)

    pc = {}
    for j in range(2):
        cols = slice(j * n_half, (j + 1) * n_half)
        for at in range(j * n_half, (j + 1) * n_half, chunk):
            some = slice(at, at + chunk)
            proj[:, some] = (dot32(att[:, :cut], out_n[:, some]) + dot32(att[:, cut:], out_w[:, some])).astype(bf16)
        for i, who in enumerate((cx_peer, c_peer)):
            pc[j, i] = send(proj.at[row_block(who), cols], core_in.at[i, :, cols],
                            pc_ss.at[j, i], pc_rs.at[j, i], {"tp": c_peer})
            pc[j, i].start()
    weights_when(0, 1, 1)
    px = []
    for j in range(2):
        cols = slice(j * n_half, (j + 1) * n_half)
        pc[j, 0].wait_recv()
        x_out[:, cols] = (proj[row_block(x_peer), cols].astype(f32) + core_in[0, :, cols].astype(f32)).astype(bf16)
        px.append(send(x_out.at[:, cols], x_in.at[:, cols], px_ss.at[j], px_rs.at[j], {"tp": x_peer}))
        px[j].start()
    answer(0, to_near_edge)
    answer(0, across_all)
    for j in range(2):
        pc[j, 1].wait_recv()
        px[j].wait_recv()
    projected = proj[row_block(t)].astype(f32) + core_in[1].astype(f32) + x_in[...].astype(f32)
    mid = (resid[...].astype(f32) + projected).astype(bf16)
    middle[...] = mid
    mid32 = mid.astype(f32)
    normed = mid32 * lax.rsqrt(jnp.mean(mid32 * mid32, axis=-1, keepdims=True) + NORM_EPS)
    act[pl.ds(s * rows + t * mine, mine)] = (normed * norm_gain[...].astype(f32)[None]).astype(bf16)

    half_mine = mine // 2
    ax, ac, az = {}, {}, {}

    def block(i, half, who):
        return act.at[pl.ds(planes[i] * rows + who * mine + half * half_mine, half_mine)]

    def spread(i, half):
        ref = block(i, half, t)
        ax[i, half] = send(ref, ref, ax_ss.at[i, half], ax_rs.at[i, half], {"tp": x_peer})
        ax[i, half].start()
        ac[i, half, 0] = send(ref, ref, ac_ss.at[i, half, 0], ac_rs.at[i, half, 0], {"tp": c_peer})
        ac[i, half, 0].start()

    def cross(i):
        for half in range(2):
            ax[i, half].wait_recv()
            ref = block(i, half, x_peer)
            ac[i, half, 1] = send(ref, ref, ac_ss.at[i, half, 1], ac_rs.at[i, half, 1], {"tp": c_peer})
            ac[i, half, 1].start()

    def next_hop(i, half):
        ref = block(i, half, t)
        return send(ref, ref, az_ss.at[i, half, 0], az_rs.at[planes[i], half], {"sp": after(i)})

    def first_hop(half, way):
        ref = block(0, half, t)
        return send(ref, ref, az_ss.at[0, half, (1 - way) // 2], az_rs.at[s, half], {"sp": s + way})

    for half in range(2):
        for way in (1, -1):
            @pl.when(ends(way))
            def _():
                first_hop(half, way).start()
        spread(0, half)
    ahead(1)

    def gather(i):
        for half in range(2):
            ref = block(i, half, t)
            send(ref, ref, az_ss.at[i, half, 1], az_rs.at[planes[i], half], {"sp": planes[i]}).wait_recv()

            @pl.when(onward(i))
            def _():
                next_hop(i, half).start()
            spread(i, half)

    def ready(i):
        for half in range(2):
            for k in range(2):
                ac[i, half, k].wait_recv()

    def lift(i):
        @typed
        def _(size):
            lifted = dot32(act[pl.ds(planes[i] * rows, rows)], up_full[:, :size])
            hidden[i, :, :size] = jnp.square(jnp.maximum(lifted, 0.0)).astype(bf16)

    rc, rx, rz = {}, {}, {}

    def lower(i, j):
        cols = cols_of(sources[j])

        @typed
        def _(size):
            part[i, :, cols] = dot32(hidden[i, :, :size], down_full[:size, cols]).astype(bf16)

        for k, who in enumerate((cx_peer, c_peer)):
            rc[i, j, k] = send(part.at[i, row_block(who), cols], core_recv.at[i, k, :, cols],
                               rc_ss.at[i, j, k], rc_rs.at[i, j, k], {"tp": c_peer})
            rc[i, j, k].start()

    def across(i, j):
        cols = cols_of(sources[j])
        rc[i, j, 0].wait_recv()
        x_send[i, :, cols] = (part[i, row_block(x_peer), cols].astype(f32)
                              + core_recv[i, 0, :, cols].astype(f32)).astype(bf16)
        rx[i, j] = send(x_send.at[i, :, cols], x_recv.at[i, :, cols], rx_ss.at[i, j], rx_rs.at[i, j], {"tp": x_peer})
        rx[i, j].start()

    def home(i, j):
        cols = cols_of(sources[j])
        rc[i, j, 1].wait_recv()
        rx[i, j].wait_recv()
        term = (part[i, row_block(t), cols].astype(f32) + core_recv[i, 1, :, cols].astype(f32)
                + x_recv[i, :, cols].astype(f32))
        if i == 0:
            total[:, cols] = term
            return
        z_send[i, :, cols] = term.astype(bf16)
        rz[i, j] = send(z_send.at[i, :, cols], z_recv.at[s, :, cols], rz_ss.at[i, j], rz_rs.at[s, sources[j]],
                        {"sp": planes[i]})
        rz[i, j].start()

    steps = []

    def run(i, j):
        lower(i, j)
        steps.append((i, j))
        if len(steps) > 1:
            across(*steps[-2])
        if len(steps) > 3:
            home(*steps[-4])

    answer(0, to_far_edge)
    weights_when(0, 0, 1)
    gather(1)
    weights_on(0, 2)
    for i in range(2, sp_n - 1):
        gather(i)
    answer(1, to_middle, wait=False)
    for i in range(3, sp_n):
        weights_on(0, i)
    cross(0)
    cross(1)
    gather(sp_n - 1)
    answer(1, to_near_edge, wait=False)
    invite(1)
    ready(0)
    noted(1)
    answer(1, to_middle, start=False)
    for i in range(1, sp_n):
        weights_in(0, i)
    lift(0)
    run(0, 0)
    weights_when(1, 1, 1)
    for i in range(1, sp_n):
        if i > 1:
            cross(i)
        ready(i)
        lift(i)
        run(i, 0)
        if i == 1:
            answer(1, to_near_edge, start=False)
            answer(1, to_far_edge)
            weights_when(1, 0, 1)
        if i + 1 < sp_n:
            weights_when(1, 1, i + 1)
    answer(1, across_all)
    for i in range(2, sp_n - 1):
        weights_when(1, 0, i)
    for j in range(1, sp_n):
        weights_in(1, j)
        for i in (list(range(1, sp_n)) + [0] if j < 3 else [3, 2, 1, 0]):
            run(i, j)
            if j == 1 and i == 0:
                weights_when(1, 0, sp_n - 1)
    across(*steps[-1])
    for step in steps[-3:]:
        home(*step)

    mixer = total[...]
    for i in range(1, sp_n):
        for j in range(sp_n):
            cols = cols_of(j)
            ref = z_recv.at[planes[i], :, cols]
            send(ref, ref, rz_ss.at[i, j], rz_rs.at[planes[i], j], {"sp": planes[i]}).wait_recv()
        mixer = mixer + z_recv[planes[i]].astype(f32)
    out[...] = (middle[...].astype(f32) + mixer).astype(bf16)

    for way in (1, -1):
        @pl.when(ends(way))
        def _():
            kv_first(way).wait_send()
    for i in range(1, sp_n):
        @pl.when(onward(i))
        def _():
            kv_next(i).wait_send()
    for half in range(2):
        for way in (1, -1):
            @pl.when(ends(way))
            def _():
                first_hop(half, way).wait_send()
        for i in range(1, sp_n):
            @pl.when(onward(i))
            def _():
                next_hop(i, half).wait_send()
    for kind in range(2):
        for i in range(1, sp_n):
            typed(lambda size: weight_send(kind, i, size).wait_send(), sources[i])
            typed(lambda size: weight_pass(kind, i, size).wait_send())
    for group in (pc, ax, ac, rc, rx, rz):
        for copy in group.values():
            copy.wait_send()
    for copy in px:
        copy.wait_send()


def shares_of(up_weight):
    half = up_weight.shape[1] // 2
    small = half * 3 // 8 // 128 * 128
    return small, half - small


def fused(sizes, resid_in, query_narrow, key_narrow, value_narrow, query_wide, key_wide, value_wide,
          lambda_narrow, lambda_wide, head_gain, out_narrow, out_wide, norm_gain, up_weight, down_weight):
    grp_n, sp_n, tp_n = sizes
    bf16, f32 = jnp.bfloat16, jnp.float32
    rows, v_width = query_narrow.shape[0], value_narrow.shape[2]
    spots, maps, flat = [], [], []
    kv_at = order = 0
    for query, key, value in ((query_narrow, key_narrow, value_narrow), (query_wide, key_wide, value_wide)):
        heads, both = query.shape[1:]
        kheads = key.shape[1]
        spots += [(kv_at, kheads * both), (kv_at + kheads * both, kheads * v_width)]
        flat += [key.reshape(rows, kheads * both), value.reshape(rows, kheads * v_width)]
        some = []
        for h in range(heads):
            kh = h // (heads // kheads)
            some.append((order, kh, both // 2, kv_at + kh * both, kv_at + kheads * both + kh * v_width))
            order += 1
        maps.append(some)
        kv_at += kheads * (both + v_width)
    mine, width = resid_in.shape
    deep, shares = up_weight.shape[0], shares_of(up_weight)
    hid = shares[1]
    vm, sm, anyw = (pl.BlockSpec(memory_space=m) for m in (pltpu.VMEM, pltpu.SMEM, pl.ANY))
    dma = pltpu.SemaphoreType.DMA
    n = sp_n
    scratch = [
        pltpu.VMEM(query_narrow.shape, bf16),
        pltpu.VMEM(query_wide.shape, bf16),
        pltpu.VMEM((2 * order, rows, 128), bf16),
        pltpu.VMEM((2 * order, rows, 1), f32),
        pltpu.VMEM((2 * order, rows, 1), f32),
        pltpu.VMEM((2 * order, rows, v_width), f32),
        pltpu.VMEM((mine, width), bf16),
        pltpu.VMEM(out_narrow.shape, bf16),
        pltpu.VMEM(out_wide.shape, bf16),
        pltpu.VMEM((n * rows, kv_at), bf16),
        pltpu.VMEM((rows, order * v_width), bf16),
        pltpu.VMEM((rows, width), bf16),
        pltpu.VMEM((2, mine, width), bf16),
        pltpu.VMEM((mine, width), bf16),
        pltpu.VMEM((mine, width), bf16),
        pltpu.VMEM((mine, width), bf16),
        pltpu.VMEM((n * rows, width), bf16),
        pltpu.VMEM((n, rows, hid), bf16),
        pltpu.VMEM((width, hid), bf16),
        pltpu.VMEM((hid, width), bf16),
        pltpu.VMEM((n, rows, width), bf16),
        pltpu.VMEM((n, 2, mine, width), bf16),
        pltpu.VMEM((n, mine, width), bf16),
        pltpu.VMEM((n, mine, width), bf16),
        pltpu.VMEM((n, mine, width), bf16),
        pltpu.VMEM((n, mine, width), bf16),
        pltpu.VMEM((mine, width), f32),
        pltpu.SemaphoreType.REGULAR((2, n)),
        dma((11,)),
        dma((n, 2)), dma((n,)),
        *(dma(k) for k in ((2, n), (2, n), (2, 2), (2,)) for _ in range(2)),
        dma((n, 2, 2)), dma((n, 2)),
        *(dma(k) for k in ((n, 2), (n, 2, 2), (n, n, 2), (n, n), (n, n)) for _ in range(2)),
    ]
    return pl.pallas_call(
        lambda *refs: layer_kernel((grp_n, sp_n, tp_n, shares, tuple(spots), tuple(maps)), *refs),
        out_shape=pltpu.VMEM(resid_in.shape, bf16),
        in_specs=[anyw] * 7 + [sm, sm, vm, anyw, anyw, vm, anyw, anyw],
        out_specs=vm,
        scratch_shapes=scratch,
        compiler_params=pltpu.CompilerParams(
            collective_id=0, has_side_effects=True, vmem_limit_bytes=VMEM_BYTES),
        name="layer",
    )(resid_in, query_narrow, flat[0], flat[1], query_wide, flat[2], flat[3], lambda_narrow, lambda_wide,
      head_gain, out_narrow, out_wide, norm_gain, up_weight, down_weight)


def fits(sizes, resid_in, query_narrow, query_wide, up_weight):
    grp_n, sp_n, tp_n = sizes
    rows, width = query_narrow.shape[0], resid_in.shape[1]
    held = 2 * width * (3 * sp_n * rows + 2 * rows + 2 * up_weight.shape[1] // sp_n)
    return (grp_n == 2 and tp_n == 4 and sp_n == 4 and up_weight.shape[1] % 1024 == 0
            and up_weight.shape[0] % 256 == 0 and resid_in.shape[0] % 32 == 0 and held < VMEM_BYTES // 2
            and query_narrow.shape[2] == 128 and query_wide.shape[2] == 256)


def solution(mesh):
    placed = (
        P(("grp", "sp", "tp"), None),
        P(("grp", "sp"), "tp", None),
        P(("grp", "sp"), "tp", None),
        P(("grp", "sp"), "tp", None),
        P(("grp", "sp"), "tp", None),
        P(("grp", "sp"), "tp", None),
        P(("grp", "sp"), "tp", None),
        P("tp"),
        P("tp"),
        P(),
        P("tp", None),
        P("tp", None),
        P(),
        P("sp", "tp"),
        P("tp", "sp"),
    )
    sizes = tuple(mesh.shape[axis] for axis in ("grp", "sp", "tp"))

    def layer(*blocks):
        if fits(sizes, blocks[0], blocks[1], blocks[4], blocks[13]):
            return fused(sizes, *blocks)
        return shards(*blocks)

    return jax.shard_map(
        layer, mesh=mesh, in_specs=placed, out_specs=P(("grp", "sp", "tp"), None), check_vma=False
    )
```

```python
import functools
import math

import jax
import jax.numpy as jnp
from jax import lax
from jax.experimental import pallas as pl
from jax.experimental.pallas import tpu as pltpu
from jax.sharding import PartitionSpec as P

NORM_EPS = 1e-06
OUT_SCALE = 0.8


def empty_state(query, key_head_stack, value_width):
    row_count, head_count = (query.shape[0], query.shape[1])
    group_size = head_count // key_head_stack
    row_top = jnp.full((key_head_stack, group_size, 2, row_count), -jnp.inf, jnp.float32)
    row_total = jnp.zeros((key_head_stack, group_size, 2, row_count), jnp.float32)
    weighted_values = jnp.zeros(
        (key_head_stack, group_size, 2, row_count, value_width), jnp.float32
    )
    return (row_top, row_total, weighted_values)


def absorb(states, query, key_rows, values):
    row_count, head_count = (query.shape[0], query.shape[1])
    key_head_stack = key_rows.shape[1]
    half_width = key_rows.shape[2] // 2
    group_size = head_count // key_head_stack
    value_width = values.shape[2]
    amount = key_rows.shape[0]
    block_rows = math.gcd(amount, 512)
    rotation_count = amount // block_rows
    grouped = query.reshape(row_count, key_head_stack, group_size, 2, half_width)
    key_block_list = key_rows.reshape(rotation_count, block_rows, key_head_stack, 2, half_width)
    value_blocks = values.reshape(rotation_count, block_rows, key_head_stack, value_width)

    def visit(running, kv_pair):
        row_top, row_total, weighted_values = running
        key_blk, value_blk = kv_pair
        scores = jnp.einsum(
            "tkgcd,skcd->kgcts", grouped, key_blk, preferred_element_type=jnp.float32
        ) * half_width ** (-0.5)
        new_top = jnp.maximum(row_top, jnp.max(scores, axis=-1))
        rescale = jnp.exp(row_top - new_top)
        powers = jnp.exp(scores - new_top[..., None])
        row_total = row_total * rescale + jnp.sum(powers, axis=-1)
        weighted_values = weighted_values * rescale[..., None] + jnp.einsum(
            "iodph,hie->iodpe",
            powers.astype(jnp.bfloat16),
            value_blk,
            preferred_element_type=jnp.float32,
        )
        return ((new_top, row_total, weighted_values), None)

    outcome, _ = lax.scan(visit, states, (key_block_list, value_blocks))
    return outcome


def finish(states, lambdas, gain_vec):
    row_top, row_total, weighted_values = states
    key_head_stack, group_size, row_count = (row_top.shape[0], row_top.shape[1], row_top.shape[3])
    value_width = weighted_values.shape[4]
    first_map = weighted_values[:, :, 0] / row_total[:, :, 0, :, None]
    second_map = weighted_values[:, :, 1] / row_total[:, :, 1, :, None]
    mixed = first_map - lambdas.reshape(key_head_stack, group_size)[:, :, None, None] * second_map
    normed = (
        mixed
        * lax.rsqrt(jnp.mean(mixed * mixed, axis=-1, keepdims=True) + NORM_EPS)
        * gain_vec
        * OUT_SCALE
    )
    normed = normed.astype(jnp.bfloat16).transpose(2, 0, 1, 3)
    return normed.reshape(row_count, key_head_stack * group_size * value_width)


def attend(
    query_narrow,
    key_narrow,
    value_narrow,
    query_wide,
    key_wide,
    value_wide,
    lambda_narrow,
    lambda_wide,
    head_gain,
):
    initial = (
        empty_state(query_narrow, key_narrow.shape[1], value_narrow.shape[2]),
        empty_state(query_wide, key_wide.shape[1], value_wide.shape[2]),
    )
    narrow_keys = lax.all_gather(key_narrow, "sp", axis=0, tiled=True)
    narrow_values = lax.all_gather(value_narrow, "sp", axis=0, tiled=True)
    wide_keys = lax.all_gather(key_wide, "sp", axis=0, tiled=True)
    wide_values = lax.all_gather(value_wide, "sp", axis=0, tiled=True)
    narrow_state = absorb(initial[0], query_narrow, narrow_keys, narrow_values)
    wide_state = absorb(initial[1], query_wide, wide_keys, wide_values)
    return (
        finish(narrow_state, lambda_narrow, head_gain),
        finish(wide_state, lambda_wide, head_gain),
    )


def shards(
    resid_in,
    query_narrow,
    key_narrow,
    value_narrow,
    query_wide,
    key_wide,
    value_wide,
    lambda_narrow,
    lambda_wide,
    head_gain,
    out_narrow,
    out_wide,
    norm_gain,
    up_weight,
    down_weight,
):
    att_narrow, att_wide = attend(
        query_narrow,
        key_narrow,
        value_narrow,
        query_wide,
        key_wide,
        value_wide,
        lambda_narrow,
        lambda_wide,
        head_gain,
    )
    projected = lax.psum_scatter(
        (
            jnp.dot(att_narrow, out_narrow, preferred_element_type=jnp.float32)
            + jnp.dot(att_wide, out_wide, preferred_element_type=jnp.float32)
        ).astype(jnp.bfloat16),
        "tp",
        scatter_dimension=0,
        tiled=True,
    ).astype(jnp.float32)
    middle = (resid_in.astype(jnp.float32) + projected).astype(jnp.bfloat16)
    middle_f32 = middle.astype(jnp.float32)
    normed = middle_f32 * lax.rsqrt(
        jnp.mean(middle_f32 * middle_f32, axis=-1, keepdims=True) + NORM_EPS
    )
    normed = (normed * norm_gain.astype(jnp.float32)).astype(jnp.bfloat16)
    whole_rows = lax.all_gather(normed, "tp", axis=0, tiled=True)
    up_collected = lax.all_gather(up_weight, "sp", axis=0, tiled=True)
    lifted = jnp.dot(whole_rows, up_collected, preferred_element_type=jnp.float32)
    activated = jnp.square(jax.nn.relu(lifted)).astype(jnp.bfloat16)
    partials = jnp.dot(
        activated,
        lax.all_gather(down_weight, "sp", axis=1, tiled=True),
        preferred_element_type=jnp.float32,
    )
    mixer_out = lax.psum_scatter(
        partials.astype(jnp.bfloat16), "tp", scatter_dimension=0, tiled=True
    ).astype(jnp.float32)
    return (middle_f32 + mixer_out).astype(jnp.bfloat16)


LOG2E = math.log2(math.e)
VMEM_BYTES = 60 * 2**20


def dot32(a, b):
    return jnp.dot(a, b, preferred_element_type=jnp.float32)


def layer_kernel(plan, resid_in, qn_in, kn_in, vn_in, qw_in, kw_in, vw_in, lam_n, lam_w, head_gain,
                 outn_in, outw_in, norm_gain, up, down,
                 out, qn, qw, queue, tops, totals, sums, resid, out_n, out_w, kv_full, att, proj, core_in, x_out, x_in, middle, act,
                 hidden, up_full, down_full, part, core_recv, x_send, x_recv, z_send, z_recv, total,
                 go, local, kv_ss, kv_rs, wz_ss, wz_rs, wy_ss, wy_rs, pc_ss, pc_rs, px_ss, px_rs,
                 az_ss, az_rs, ax_ss, ax_rs, ac_ss, ac_rs, rc_ss, rc_rs, rx_ss, rx_rs, rz_ss, rz_rs):
    grp_n, sp_n, tp_n, shares, spots, maps = plan
    g, s, t = lax.axis_index("grp"), lax.axis_index("sp"), lax.axis_index("tp")
    rows = qn.shape[0]
    mine, width = resid.shape
    deep = up.shape[0]
    f32, bf16 = jnp.float32, jnp.bfloat16
    x_peer = lax.rem(t + 2, tp_n)
    c_peer = t + 1 - 2 * lax.rem(t, 2)
    cx_peer = lax.rem(c_peer + 2, tp_n)
    y_peer = 1 - g

    def by_distance(sign):
        lists = [sorted(range(sp_n), key=lambda p: (abs(p - me), sign * abs(2 * p + 1 - sp_n)))
                 for me in range(sp_n)]
        found = [s]
        for i in range(1, sp_n):
            at = lists[0][i]
            for me in range(1, sp_n):
                at = jnp.where(s == me, lists[me][i], at)
            found.append(at)
        return found

    planes, sources = by_distance(1), by_distance(-1)

    def send(src, dst, ss, rs, dev):
        return pltpu.make_async_remote_copy(
            src_ref=src, dst_ref=dst, send_sem=ss, recv_sem=rs,
            device_id=dev, device_id_type=pl.DeviceIdType.MESH)

    def cols_of(p):
        return pl.ds(pl.multiple_of(p * deep, 128), deep)

    loads = []

    def load(src, dst):
        copy = pltpu.make_async_copy(src, dst, local.at[len(loads)])
        copy.start()
        loads.append(copy)

    own = pl.ds(s * rows, rows)
    for ref, (at, size) in zip((kn_in, vn_in, kw_in, vw_in), spots):
        load(ref, kv_full.at[own, at:at + size])
    load(qn_in, qn)
    load(qw_in, qw)
    load(outn_in, out_n)
    load(outw_in, out_w)
    load(resid_in, resid)
    edge = (s == 0) | (s == sp_n - 1)
    middle_plane = jnp.logical_not(edge)

    def typed(body, p=None):
        at_edge = edge if p is None else (p == 0) | (p == sp_n - 1)
        for when, size in ((at_edge, shares[0]), (jnp.logical_not(at_edge), shares[1])):
            @pl.when(when)
            def _():
                body(size)

    def first_unit(p):
        return pl.multiple_of(p * shares[1] - jnp.where(p > 0, shares[1] - shares[0], 0), 128)

    def own_weights(size):
        units = pl.ds(first_unit(s), size)
        return (pltpu.make_async_copy(up.at[:, units], up_full.at[pl.ds(s * deep, deep), :size], local.at[9]),
                pltpu.make_async_copy(down.at[units], down_full.at[:size, cols_of(s)], local.at[10]))

    @typed
    def _(size):
        for copy in own_weights(size):
            copy.start()


    barrier = pltpu.get_barrier_semaphore()
    peers = [{"sp": lax.rem(s + d, sp_n)} for d in range(1, sp_n)]
    peers += [{"sp": lax.rem(s + d, sp_n), "tp": c_peer} for d in range(1, sp_n)]
    peers += [{"tp": x_peer}, {"tp": c_peer}, {"grp": y_peer}]
    for peer in peers:
        pl.semaphore_signal(barrier, inc=1, device_id=peer, device_id_type=pl.DeviceIdType.MESH)
    for copy in loads[:4]:
        copy.wait()
    pl.semaphore_wait(barrier, len(peers))

    half_d = deep // grp_n

    def weight_send(kind, i, size):
        to = sources[i]
        if kind == 0:
            return send(up.at[pl.ds(g * half_d, half_d), pl.ds(first_unit(to), size)],
                        up_full.at[pl.ds(s * deep + g * half_d, half_d), :size],
                        wz_ss.at[0, i], wz_rs.at[0, s], {"sp": to})
        half_h = size // grp_n
        return send(down.at[pl.ds(first_unit(to) + g * half_h, half_h)],
                    down_full.at[pl.ds(g * half_h, half_h), cols_of(s)],
                    wz_ss.at[1, i], wz_rs.at[1, s], {"sp": to})

    def weight_ref(kind, i, size):
        at = sources[i]
        if kind == 0:
            return up_full.at[pl.ds(at * deep + g * half_d, half_d), :size]
        half_h = size // grp_n
        return down_full.at[pl.ds(g * half_h, half_h), cols_of(at)]

    def weight_pass(kind, i, size):
        ref = weight_ref(kind, i, size)
        return send(ref, ref, wy_ss.at[kind, i], wy_rs.at[kind, i], {"grp": y_peer})

    def weights_begin(kind, i):
        typed(lambda size: weight_send(kind, i, size).start(), sources[i])

    def weights_in(kind, i):
        typed(lambda size: weight_pass(kind, i, size).wait_recv())

    def weights_got(kind, i, size):
        ref = weight_ref(kind, i, size)
        send(ref, ref, wz_ss.at[kind, i], wz_rs.at[kind, sources[i]], {"sp": sources[i]}).wait_recv()
        weight_pass(kind, i, size).start()

    def weights_on(kind, i):
        typed(lambda size: weights_got(kind, i, size))

    def weights_when(kind, where, i):
        @pl.when((edge, middle_plane)[where])
        def _():
            weights_got(kind, i, shares[where])

    def ends(way):
        return (s < sp_n - 1) if way == 1 else (s > 0)

    def onward(i):
        return ((planes[i] < s) & (s < sp_n - 1)) | ((planes[i] > s) & (s > 0))

    def after(i):
        return jnp.clip(jnp.where(planes[i] < s, s + 1, s - 1), 0, sp_n - 1)

    def invite(kind):
        for i in range(1, sp_n):
            for who in (t, c_peer):
                pl.semaphore_signal(go.at[kind, s], inc=1, device_id={"sp": sources[i], "tp": who},
                                    device_id_type=pl.DeviceIdType.MESH)

    def answer(kind, when, wait=True, start=True):
        for i in range(1, sp_n):
            ahead_of = edge if i == 1 else False

            @pl.when(when(sources[i]) & jnp.logical_not(ahead_of))
            def _():
                if wait:
                    pl.semaphore_wait(go.at[kind, sources[i]], 2)
                if start:
                    weights_begin(kind, i)

    def ahead(kind):
        @pl.when(edge)
        def _():
            weights_begin(kind, 1)

    def is_edge(p):
        return (p == 0) | (p == sp_n - 1)

    def near(p):
        return (p == s + 1) | (p == s - 1)

    def to_middle(p):
        return jnp.logical_not(is_edge(p))

    def to_near_edge(p):
        return is_edge(p) & middle_plane & near(p)

    def to_far_edge(p):
        return is_edge(p) & middle_plane & jnp.logical_not(near(p))

    def across_all(p):
        return is_edge(p) & edge

    def noted(kind):
        @pl.when(edge)
        def _():
            pl.semaphore_wait(go.at[kind, sources[1]], 2)

    def keys_of(p):
        return kv_full.at[pl.ds(p * rows, rows)]

    def kv_first(way):
        return send(keys_of(s), keys_of(s), kv_ss.at[0, (1 - way) // 2], kv_rs.at[s], {"sp": s + way})

    def kv_next(i):
        ref = keys_of(planes[i])
        return send(ref, ref, kv_ss.at[i, 0], kv_rs.at[planes[i]], {"sp": after(i)})

    def kv_get(i):
        ref = keys_of(planes[i])
        send(ref, ref, kv_ss.at[i, 1], kv_rs.at[planes[i]], {"sp": planes[i]}).wait_recv()

        @pl.when(onward(i))
        def _():
            kv_next(i).start()

    for way in (1, -1):
        @pl.when(ends(way))
        def _():
            kv_first(way).start()
    ahead(0)

    for copy in loads[4:6]:
        copy.wait()
    lane = lax.broadcasted_iota(jnp.int32, (rows, 128), 1)
    spot = 0
    for kind, ref in enumerate((qn, qw)):
        queries = ref[...].astype(f32)
        for h in range(len(maps[kind])):
            half = maps[kind][h][2]
            for c in range(2):
                if half < 128:
                    queue[spot] = jnp.where((lane // half) == c, queries[:, h, :], 0.0).astype(bf16)
                else:
                    queue[spot] = queries[:, h, c * half:(c + 1) * half].astype(bf16)
                spot += 1

    def attend(blocks, final):
        spot = 0
        work = []
        for kind in range(2):
            for h, (order, kh, half, k_at, v_at) in enumerate(maps[kind]):
                for c in range(2):
                    key_at = k_at + (c * half if half == 128 else 0)
                    scores = [lax.dot_general(
                        queue[spot], kv_full[pl.ds(p * rows, rows), key_at:key_at + 128],
                        (((1,), (1,)), ((), ())), preferred_element_type=f32) for p in blocks]
                    top = jnp.max(functools.reduce(jnp.maximum, scores), axis=-1, keepdims=True)
                    work.append((scores, top, half ** -0.5 * LOG2E, v_at))
                    spot += 1
        sides = []
        for spot, (scores, top, scale, v_at) in enumerate(work):
            if final:
                before = tops[spot]
                top = jnp.maximum(top, before)
            powers = [jnp.exp2((one - top) * scale) for one in scores]
            row_total = jnp.sum(functools.reduce(jnp.add, powers), axis=-1, keepdims=True)
            summed = functools.reduce(jnp.add, [
                dot32(one.astype(bf16), kv_full[pl.ds(p * rows, rows), v_at:v_at + head_gain.shape[0]])
                for p, one in zip(blocks, powers)])
            if final:
                fade = jnp.exp2((before - top) * scale)
                sides.append((summed + sums[spot] * fade) * (1.0 / (row_total + totals[spot] * fade)))
            else:
                tops[spot] = top
                totals[spot] = row_total
                sums[spot] = summed
        spot = 0
        for kind in range(2):
            for h, (order, *_) in enumerate(maps[kind] if final else ()):
                lam = (lam_n if kind == 0 else lam_w)[h]
                mixed = sides[2 * order] - lam * sides[2 * order + 1]
                v_width = mixed.shape[1]
                normed = (mixed * lax.rsqrt(jnp.mean(mixed * mixed, axis=-1, keepdims=True) + NORM_EPS)
                          * (head_gain[...][None] * OUT_SCALE))
                att[:, order * v_width:(order + 1) * v_width] = normed.astype(bf16)

    for i in range(1, sp_n - 1):
        kv_get(i)
    answer(0, lambda p: to_middle(p) & edge, wait=False)
    attend(planes[:sp_n - 1], False)
    noted(0)
    answer(0, lambda p: to_middle(p) & edge, start=False)
    kv_get(sp_n - 1)
    invite(0)
    answer(0, lambda p: to_middle(p) & middle_plane, wait=False)
    attend(planes[sp_n - 1:], True)
    answer(0, lambda p: to_middle(p) & middle_plane, start=False)
    for copy in loads[6:]:
        copy.wait()

    @typed
    def _(size):
        for copy in own_weights(size):
            copy.wait()


    cut = out_n.shape[0]
    chunk = math.gcd(width, 512)
    n_half = width // 2

    def row_block(who):
        return pl.ds(who * mine, mine)

    pc = {}
    for j in range(2):
        cols = slice(j * n_half, (j + 1) * n_half)
        for at in range(j * n_half, (j + 1) * n_half, chunk):
            some = slice(at, at + chunk)
            proj[:, some] = (dot32(att[:, :cut], out_n[:, some]) + dot32(att[:, cut:], out_w[:, some])).astype(bf16)
        for i, who in enumerate((cx_peer, c_peer)):
            pc[j, i] = send(proj.at[row_block(who), cols], core_in.at[i, :, cols],
                            pc_ss.at[j, i], pc_rs.at[j, i], {"tp": c_peer})
            pc[j, i].start()
    weights_when(0, 1, 1)
    px = []
    for j in range(2):
        cols = slice(j * n_half, (j + 1) * n_half)
        pc[j, 0].wait_recv()
        x_out[:, cols] = (proj[row_block(x_peer), cols].astype(f32) + core_in[0, :, cols].astype(f32)).astype(bf16)
        px.append(send(x_out.at[:, cols], x_in.at[:, cols], px_ss.at[j], px_rs.at[j], {"tp": x_peer}))
        px[j].start()
    answer(0, to_near_edge)
    answer(0, across_all)
    for j in range(2):
        pc[j, 1].wait_recv()
        px[j].wait_recv()
    projected = proj[row_block(t)].astype(f32) + core_in[1].astype(f32) + x_in[...].astype(f32)
    mid = (resid[...].astype(f32) + projected).astype(bf16)
    middle[...] = mid
    mid32 = mid.astype(f32)
    normed = mid32 * lax.rsqrt(jnp.mean(mid32 * mid32, axis=-1, keepdims=True) + NORM_EPS)
    act[pl.ds(s * rows + t * mine, mine)] = (normed * norm_gain[...].astype(f32)[None]).astype(bf16)

    half_mine = mine // 2
    ax, ac, az = {}, {}, {}

    def block(i, half, who):
        return act.at[pl.ds(planes[i] * rows + who * mine + half * half_mine, half_mine)]

    def spread(i, half):
        ref = block(i, half, t)
        ax[i, half] = send(ref, ref, ax_ss.at[i, half], ax_rs.at[i, half], {"tp": x_peer})
        ax[i, half].start()
        ac[i, half, 0] = send(ref, ref, ac_ss.at[i, half, 0], ac_rs.at[i, half, 0], {"tp": c_peer})
        ac[i, half, 0].start()

    def cross(i):
        for half in range(2):
            ax[i, half].wait_recv()
            ref = block(i, half, x_peer)
            ac[i, half, 1] = send(ref, ref, ac_ss.at[i, half, 1], ac_rs.at[i, half, 1], {"tp": c_peer})
            ac[i, half, 1].start()

    def next_hop(i, half):
        ref = block(i, half, t)
        return send(ref, ref, az_ss.at[i, half, 0], az_rs.at[planes[i], half], {"sp": after(i)})

    def first_hop(half, way):
        ref = block(0, half, t)
        return send(ref, ref, az_ss.at[0, half, (1 - way) // 2], az_rs.at[s, half], {"sp": s + way})

    for half in range(2):
        for way in (1, -1):
            @pl.when(ends(way))
            def _():
                first_hop(half, way).start()
        spread(0, half)
    ahead(1)

    def gather(i):
        for half in range(2):
            ref = block(i, half, t)
            send(ref, ref, az_ss.at[i, half, 1], az_rs.at[planes[i], half], {"sp": planes[i]}).wait_recv()

            @pl.when(onward(i))
            def _():
                next_hop(i, half).start()
            spread(i, half)

    def ready(i):
        for half in range(2):
            for k in range(2):
                ac[i, half, k].wait_recv()

    def lift(i):
        @typed
        def _(size):
            lifted = dot32(act[pl.ds(planes[i] * rows, rows)], up_full[:, :size])
            hidden[i, :, :size] = jnp.square(jnp.maximum(lifted, 0.0)).astype(bf16)

    rc, rx, rz = {}, {}, {}

    def lower(i, j):
        cols = cols_of(sources[j])

        @typed
        def _(size):
            part[i, :, cols] = dot32(hidden[i, :, :size], down_full[:size, cols]).astype(bf16)

        for k, who in enumerate((cx_peer, c_peer)):
            rc[i, j, k] = send(part.at[i, row_block(who), cols], core_recv.at[i, k, :, cols],
                               rc_ss.at[i, j, k], rc_rs.at[i, j, k], {"tp": c_peer})
            rc[i, j, k].start()

    def across(i, j):
        cols = cols_of(sources[j])
        rc[i, j, 0].wait_recv()
        x_send[i, :, cols] = (part[i, row_block(x_peer), cols].astype(f32)
                              + core_recv[i, 0, :, cols].astype(f32)).astype(bf16)
        rx[i, j] = send(x_send.at[i, :, cols], x_recv.at[i, :, cols], rx_ss.at[i, j], rx_rs.at[i, j], {"tp": x_peer})
        rx[i, j].start()

    def home(i, j):
        cols = cols_of(sources[j])
        rc[i, j, 1].wait_recv()
        rx[i, j].wait_recv()
        term = (part[i, row_block(t), cols].astype(f32) + core_recv[i, 1, :, cols].astype(f32)
                + x_recv[i, :, cols].astype(f32))
        if i == 0:
            total[:, cols] = term
            return
        z_send[i, :, cols] = term.astype(bf16)
        rz[i, j] = send(z_send.at[i, :, cols], z_recv.at[s, :, cols], rz_ss.at[i, j], rz_rs.at[s, sources[j]],
                        {"sp": planes[i]})
        rz[i, j].start()

    steps = []

    def run(i, j):
        lower(i, j)
        steps.append((i, j))
        if len(steps) > 1:
            across(*steps[-2])
        if len(steps) > 3:
            home(*steps[-4])

    answer(0, to_far_edge)
    weights_when(0, 0, 1)
    gather(1)
    weights_on(0, 2)
    for i in range(2, sp_n - 1):
        gather(i)
    answer(1, to_middle, wait=False)
    for i in range(3, sp_n):
        weights_on(0, i)
    cross(0)
    cross(1)
    gather(sp_n - 1)
    answer(1, to_near_edge, wait=False)
    invite(1)
    ready(0)
    noted(1)
    answer(1, to_middle, start=False)
    for i in range(1, sp_n):
        weights_in(0, i)
    lift(0)
    run(0, 0)
    weights_when(1, 1, 1)
    for i in range(1, sp_n):
        if i > 1:
            cross(i)
        ready(i)
        lift(i)
        run(i, 0)
        if i == 1:
            answer(1, to_near_edge, start=False)
            answer(1, to_far_edge)
            weights_when(1, 0, 1)
        if i + 1 < sp_n:
            weights_when(1, 1, i + 1)
    answer(1, across_all)
    for i in range(2, sp_n - 1):
        weights_when(1, 0, i)
    for j in range(1, sp_n):
        weights_in(1, j)
        for i in (list(range(1, sp_n)) + [0] if j < 3 else [3, 2, 1, 0]):
            run(i, j)
            if j == 1 and i == 0:
                weights_when(1, 0, sp_n - 1)
    across(*steps[-1])
    for step in steps[-3:]:
        home(*step)

    mixer = total[...]
    for i in range(1, sp_n):
        for j in range(sp_n):
            cols = cols_of(j)
            ref = z_recv.at[planes[i], :, cols]
            send(ref, ref, rz_ss.at[i, j], rz_rs.at[planes[i], j], {"sp": planes[i]}).wait_recv()
        mixer = mixer + z_recv[planes[i]].astype(f32)
    out[...] = (middle[...].astype(f32) + mixer).astype(bf16)

    for way in (1, -1):
        @pl.when(ends(way))
        def _():
            kv_first(way).wait_send()
    for i in range(1, sp_n):
        @pl.when(onward(i))
        def _():
            kv_next(i).wait_send()
    for half in range(2):
        for way in (1, -1):
            @pl.when(ends(way))
            def _():
                first_hop(half, way).wait_send()
        for i in range(1, sp_n):
            @pl.when(onward(i))
            def _():
                next_hop(i, half).wait_send()
    for kind in range(2):
        for i in range(1, sp_n):
            typed(lambda size: weight_send(kind, i, size).wait_send(), sources[i])
            typed(lambda size: weight_pass(kind, i, size).wait_send())
    for group in (pc, ax, ac, rc, rx, rz):
        for copy in group.values():
            copy.wait_send()
    for copy in px:
        copy.wait_send()


def shares_of(up_weight):
    half = up_weight.shape[1] // 2
    small = half * 3 // 8 // 128 * 128
    return small, half - small


def fused(sizes, resid_in, query_narrow, key_narrow, value_narrow, query_wide, key_wide, value_wide,
          lambda_narrow, lambda_wide, head_gain, out_narrow, out_wide, norm_gain, up_weight, down_weight):
    grp_n, sp_n, tp_n = sizes
    bf16, f32 = jnp.bfloat16, jnp.float32
    rows, v_width = query_narrow.shape[0], value_narrow.shape[2]
    spots, maps, flat = [], [], []
    kv_at = order = 0
    for query, key, value in ((query_narrow, key_narrow, value_narrow), (query_wide, key_wide, value_wide)):
        heads, both = query.shape[1:]
        kheads = key.shape[1]
        spots += [(kv_at, kheads * both), (kv_at + kheads * both, kheads * v_width)]
        flat += [key.reshape(rows, kheads * both), value.reshape(rows, kheads * v_width)]
        some = []
        for h in range(heads):
            kh = h // (heads // kheads)
            some.append((order, kh, both // 2, kv_at + kh * both, kv_at + kheads * both + kh * v_width))
            order += 1
        maps.append(some)
        kv_at += kheads * (both + v_width)
    mine, width = resid_in.shape
    deep, shares = up_weight.shape[0], shares_of(up_weight)
    hid = shares[1]
    vm, sm, anyw = (pl.BlockSpec(memory_space=m) for m in (pltpu.VMEM, pltpu.SMEM, pl.ANY))
    dma = pltpu.SemaphoreType.DMA
    n = sp_n
    scratch = [
        pltpu.VMEM(query_narrow.shape, bf16),
        pltpu.VMEM(query_wide.shape, bf16),
        pltpu.VMEM((2 * order, rows, 128), bf16),
        pltpu.VMEM((2 * order, rows, 1), f32),
        pltpu.VMEM((2 * order, rows, 1), f32),
        pltpu.VMEM((2 * order, rows, v_width), f32),
        pltpu.VMEM((mine, width), bf16),
        pltpu.VMEM(out_narrow.shape, bf16),
        pltpu.VMEM(out_wide.shape, bf16),
        pltpu.VMEM((n * rows, kv_at), bf16),
        pltpu.VMEM((rows, order * v_width), bf16),
        pltpu.VMEM((rows, width), bf16),
        pltpu.VMEM((2, mine, width), bf16),
        pltpu.VMEM((mine, width), bf16),
        pltpu.VMEM((mine, width), bf16),
        pltpu.VMEM((mine, width), bf16),
        pltpu.VMEM((n * rows, width), bf16),
        pltpu.VMEM((n, rows, hid), bf16),
        pltpu.VMEM((width, hid), bf16),
        pltpu.VMEM((hid, width), bf16),
        pltpu.VMEM((n, rows, width), bf16),
        pltpu.VMEM((n, 2, mine, width), bf16),
        pltpu.VMEM((n, mine, width), bf16),
        pltpu.VMEM((n, mine, width), bf16),
        pltpu.VMEM((n, mine, width), bf16),
        pltpu.VMEM((n, mine, width), bf16),
        pltpu.VMEM((mine, width), f32),
        pltpu.SemaphoreType.REGULAR((2, n)),
        dma((11,)),
        dma((n, 2)), dma((n,)),
        *(dma(k) for k in ((2, n), (2, n), (2, 2), (2,)) for _ in range(2)),
        dma((n, 2, 2)), dma((n, 2)),
        *(dma(k) for k in ((n, 2), (n, 2, 2), (n, n, 2), (n, n), (n, n)) for _ in range(2)),
    ]
    return pl.pallas_call(
        lambda *refs: layer_kernel((grp_n, sp_n, tp_n, shares, tuple(spots), tuple(maps)), *refs),
        out_shape=pltpu.VMEM(resid_in.shape, bf16),
        in_specs=[anyw] * 7 + [sm, sm, vm, anyw, anyw, vm, anyw, anyw],
        out_specs=vm,
        scratch_shapes=scratch,
        compiler_params=pltpu.CompilerParams(
            collective_id=0, has_side_effects=True, vmem_limit_bytes=VMEM_BYTES),
        name="layer",
    )(resid_in, query_narrow, flat[0], flat[1], query_wide, flat[2], flat[3], lambda_narrow, lambda_wide,
      head_gain, out_narrow, out_wide, norm_gain, up_weight, down_weight)


def fits(sizes, resid_in, query_narrow, query_wide, up_weight):
    grp_n, sp_n, tp_n = sizes
    rows, width = query_narrow.shape[0], resid_in.shape[1]
    held = 2 * width * (3 * sp_n * rows + 2 * rows + 2 * up_weight.shape[1] // sp_n)
    return (grp_n == 2 and tp_n == 4 and sp_n == 4 and up_weight.shape[1] % 1024 == 0
            and up_weight.shape[0] % 256 == 0 and resid_in.shape[0] % 32 == 0 and held < VMEM_BYTES // 2
            and query_narrow.shape[2] == 128 and query_wide.shape[2] == 256)


def solution(mesh):
    placed = (
        P(("grp", "sp", "tp"), None),
        P(("grp", "sp"), "tp", None),
        P(("grp", "sp"), "tp", None),
        P(("grp", "sp"), "tp", None),
        P(("grp", "sp"), "tp", None),
        P(("grp", "sp"), "tp", None),
        P(("grp", "sp"), "tp", None),
        P("tp"),
        P("tp"),
        P(),
        P("tp", None),
        P("tp", None),
        P(),
        P("sp", "tp"),
        P("tp", "sp"),
    )
    sizes = tuple(mesh.shape[axis] for axis in ("grp", "sp", "tp"))

    def layer(*blocks):
        if fits(sizes, blocks[0], blocks[1], blocks[4], blocks[13]):
            return fused(sizes, *blocks)
        return shards(*blocks)

    return jax.shard_map(
        layer, mesh=mesh, in_specs=placed, out_specs=P(("grp", "sp", "tp"), None), check_vma=False
    )
```
